32 devices in a mesh: sp: 4 (over y, x), tp: 8 (over z, core).
Axes of the slice: x: 2, y: 2, z: 4, core: 2. Of those that a mesh axis runs over, the one named last changes fastest.
Arguments:
- queries: bfloat16 [3072, 16, 128], P('sp', 'tp'), may hold values from -240 to 240
- key_pairs: bfloat16 [3072, 16, 128], P('sp', 'tp'), may hold values from -11 to 11
- head_values: bfloat16 [3072, 16, 128], P('sp', 'tp'), may hold values from -6 to 6
- lambdas: float32 [16], P('tp'), may hold values from 0.3 to 0.8
- head_gain: float32 [128], replicated, may hold values from 0.1 to 1.9
- out_weight: bfloat16 [2048, 2048], replicated, may hold values from -0.125 to 0.125
- residual: bfloat16 [3072, 2048], P(('sp', 'tp')), may hold values from -6 to 6
- norm_gain: float32 [2048], replicated, may hold values from 0.1 to 1.9
- expert_ids: int32 [3072, 2], P(('sp', 'tp')), may hold values from 0 to 7, all different within a row; in each aligned block of 96 rows (0 to 95, 96 to 191, ...) at most 32 rows name the same one
- route_weights: float32 [3072, 2], P(('sp', 'tp')), may hold values from 0.2 to 1
- gate_weight: bfloat16 [8, 2048, 2048], P('sp', None, 'tp'), may hold values from -0.125 to 0.125
- up_weight: bfloat16 [8, 2048, 2048], P('sp', None, 'tp'), may hold values from -0.125 to 0.125
- down_weight: bfloat16 [8, 2048, 2048], P('sp', 'tp'), may hold values from -0.125 to 0.125
Outputs:
- merged: bfloat16 [3072, 2048], P(('sp', 'tp'))
The draws below stay inside these ranges and needn't reach their ends.
Inputs may be any that keep to these rules, and one draw needn't show every extreme that they name: `expert_ids`: within the rows of one device each expert is named at most 32 times, and exactly 32 times in some device.
All inputs are finite; a program needn't handle non-finite values.
Results may differ from the reference program's by a relative error of at most 0.019.
Values may be sent and summed in bfloat16 or wider, within the bound.
No kernel may reach another device: no remote copies, remote signals or barrier semaphores. Data moves between devices by JAX's collectives and lax.ppermute only.
A program may use at most 128 MiB of HBM per device.

```python
import math
import jax
import jax.numpy as jnp
import numpy as np
from jax import lax

D = 2048
HEADS = 16
HD = 64
VD = 128
FF = 2048
TOPK = 2
LENGTH = 3072
ROWS = 96
EXPERTS = 8
CAP = 32
N_TP = 8


def base_field(key, salt_value):
    return jnp.clip(jax.random.normal(jax.random.fold_in(key, salt_value), (LENGTH, HEADS, 2 * HD), jnp.float32), -4.0, 4.0) * 1.3


def draw_key_pairs(key, part):
    drawn_field = base_field(key, 11)
    return drawn_field.astype(jnp.bfloat16)


def draw_queries(key, part):
    drawn_field = base_field(key, 12)
    return drawn_field.astype(jnp.bfloat16)


def block_levels(rng, dims, shards, smallest, largest):
    loudness = 1.0
    for dim, blocks in shards:
        draws = jax.random.uniform(jax.random.fold_in(jax.random.fold_in(rng, 6), dim), (blocks,), jnp.float32, smallest / len(shards), largest / len(shards))
        loudness = loudness * jnp.repeat(jnp.exp(draws), dims[dim] // blocks).reshape((-1,) + (1,) * (len(dims) - 1 - dim))
    return loudness


def shared_out(own_key, own, number, rows, amount, top, limit, lean):
    order = jax.random.permutation(own_key, amount)
    crowded, common = load_shares(amount, rows * top, limit, lean, True), load_shares(amount, rows * top, limit, lean, False)
    places = jnp.arange(amount)

    def named(sizes, rotation):
        used = int((sizes > 0).sum())
        fixed = max(1, used // 4)
        passed = fixed + (places - fixed + rotation * (used - fixed)) % max(1, amount - fixed)
        return jnp.zeros((amount,), jnp.int32).at[order[jnp.where(places < fixed, places, passed)]].set(jnp.asarray(sizes, jnp.int32))

    sizes = jnp.where(number % 4 == 0, named(crowded, number // 4), named(common, number - number // 4 - 1))
    mixed = jax.random.permutation(jax.random.fold_in(own, 3), amount)
    source_of, sink = mixed[0:amount // 2 * 2:2], mixed[1:amount // 2 * 2:2]
    room = jnp.minimum(sizes[source_of] - 1, limit - sizes[sink]) // 2
    room = jnp.where((source_of == order[0]) | (sink == order[0]) | (sizes[sink] == 0), 0, jnp.maximum(room, 0))
    passed = jax.random.randint(jax.random.fold_in(own, 4), (amount // 2,), 0, 1 << 20) % (room + 1)
    sizes = sizes.at[source_of].add(-passed).at[sink].add(passed)
    items = jnp.searchsorted(jnp.cumsum(sizes), jnp.arange(rows * top), side="right").astype(jnp.int32)
    table = items.reshape(top, rows).T
    table = table[jax.random.permutation(jax.random.fold_in(own, 1), rows)]
    rotation = jax.random.randint(jax.random.fold_in(own, 2), (rows, 1), 0, top)
    return jnp.take_along_axis(table, (jnp.arange(top)[None, :] + rotation) % top, axis=1)


def load_shares(count, total, limit, skew, full):
    portions = [(1 << 20) // math.isqrt(grade ** skew) + 1 for grade in range(1, count + 1)]
    largest = limit if full else min(limit, max(-(-total // count), total * portions[0] // sum(portions)))
    least = 1 if total - largest >= count - 1 else 0
    holding, surplus = [largest] + [least] * (count - 1), total - largest - least * (count - 1)
    while surplus > 0:
        free = [i for i in range(1, count) if holding[i] < largest] or [i for i in range(1, count) if holding[i] < limit]
        mass, budget = sum([portions[i] for i in free]), surplus
        for i in free:
            more = min(limit - holding[i], max(1, budget * portions[i] // mass), surplus)
            holding[i] = holding[i] + more
            surplus = surplus - more
    return np.array(holding)


def centred(own_key, extent, scale, most, cuts=(), kind=jnp.bfloat16):
    loudness = block_levels(own_key, extent, cuts, -0.22, 0.18) if cuts else 1.0
    values = jax.random.normal(own_key, extent, jnp.float32) * scale * loudness
    return jnp.minimum(jnp.maximum(values, -most), most).astype(kind)


def setup_inputs(seed: int = 0) -> dict:
    key_list = jax.random.split(jax.random.key(seed), 14)
    queries = draw_queries(jax.random.fold_in(key_list[13], 71), 0)
    key_pairs = draw_key_pairs(jax.random.fold_in(key_list[13], 71), 0)
    head_values = centred(key_list[2], (LENGTH, HEADS, VD), 1.0, 6.0, ((0, 4), (1, 8)))
    lambdas = jnp.clip(0.3 + 0.5 * jax.random.uniform(key_list[3], (HEADS,), jnp.float32) ** block_levels(key_list[3], (HEADS,), ((0, 8),), -0.2, 0.2), 0.3, 0.8)
    head_gain = jnp.clip(1.0 + 0.18 * jax.random.normal(key_list[4], (VD,), jnp.float32), 0.1, 1.9)
    out_weight = centred(key_list[5], (HEADS * VD, D), (HEADS * VD) ** -0.5, 0.125)
    residual = centred(key_list[6], (LENGTH, D), 1.0, 6.0, ((0, 32),))
    norm_gain = jnp.clip(1.0 + 0.18 * jax.random.normal(key_list[7], (D,), jnp.float32), 0.1, 1.9)
    expert_ids_keys = jax.random.split(jax.random.fold_in(key_list[8], 1), LENGTH // ROWS)
    expert_ids_turns = jax.random.permutation(jax.random.fold_in(key_list[8], 3), LENGTH // ROWS)
    expert_ids = jax.vmap(lambda own, number: shared_out(jax.random.fold_in(key_list[8], 2), own, number, ROWS, EXPERTS, TOPK, CAP, 1))(expert_ids_keys, expert_ids_turns).reshape((LENGTH, TOPK))
    route_weights = jnp.clip(0.2 + 0.8 * jax.random.uniform(key_list[9], (LENGTH, TOPK), jnp.float32) ** block_levels(key_list[9], (LENGTH, TOPK), ((0, 32),), -0.2, 0.2), 0.2, 1.0)
    gate_weight = centred(key_list[10], (EXPERTS, D, FF), D ** -0.5, 0.125, ((0, 4), (2, 8)))
    up_weight = centred(key_list[11], (EXPERTS, D, FF), D ** -0.5, 0.125, ((0, 4), (2, 8)))
    down_weight = centred(key_list[12], (EXPERTS, FF, D), FF ** -0.5, 0.125, ((0, 4), (1, 8)))
    return {"queries": queries, "key_pairs": key_pairs, "head_values": head_values, "lambdas": lambdas, "head_gain": head_gain, "out_weight": out_weight, "residual": residual, "norm_gain": norm_gain, "expert_ids": expert_ids, "route_weights": route_weights, "gate_weight": gate_weight, "up_weight": up_weight, "down_weight": down_weight}


def attend_head(query_rows, key_rows, value_rows, weight_two):
    block_rows = min(512, LENGTH)
    columns = jnp.arange(LENGTH, dtype=jnp.int32)

    def one_block(block_index):
        offset = block_index * block_rows
        query_block = lax.dynamic_slice_in_dim(query_rows, offset, block_rows, 0)
        positions = offset + jnp.arange(block_rows, dtype=jnp.int32)
        allowed = columns[None, :] <= positions[:, None]
        results = []
        for member in range(2):
            first_col = member * HD
            scores = jnp.dot(query_block[:, first_col:first_col + HD], key_rows[:, first_col:first_col + HD].T, preferred_element_type=jnp.float32) * HD ** (-0.5)
            scores = jnp.where(allowed, scores, -jnp.inf)
            highest = lax.optimization_barrier(jnp.max(scores, axis=1, keepdims=True))
            weights = jnp.exp(scores - highest)
            totals = lax.optimization_barrier(jnp.sum(weights, axis=1, keepdims=True))
            summed = jnp.dot(weights.astype(jnp.bfloat16), value_rows, preferred_element_type=jnp.float32)
            results.append(summed / totals)
        return results[0] - weight_two * results[1]
    blocks = lax.map(one_block, jnp.arange(LENGTH // block_rows, dtype=jnp.int32))
    return blocks.reshape(LENGTH, VD)

def reference(queries, key_pairs, head_values, lambdas, head_gain, out_weight, residual, norm_gain, expert_ids, route_weights, gate_weight, up_weight, down_weight):

    def one_head(packed):
        query_rows, key_rows, value_rows, weight_two = packed
        mixed = attend_head(query_rows, key_rows, value_rows, weight_two)
        row_scale = lax.rsqrt(lax.optimization_barrier(jnp.mean(mixed * mixed, axis=1, keepdims=True)) + 1e-06)
        return (mixed * row_scale * head_gain).astype(jnp.bfloat16)
    per_head = lax.map(one_head, (jnp.transpose(queries, (1, 0, 2)), jnp.transpose(key_pairs, (1, 0, 2)), jnp.transpose(head_values, (1, 0, 2)), lambdas))
    attended = jnp.transpose(per_head, (1, 0, 2)).reshape(LENGTH, HEADS * VD)
    projected = jnp.dot(attended, out_weight, preferred_element_type=jnp.float32)
    updated = (residual.astype(jnp.float32) + projected).astype(jnp.bfloat16)
    widened = updated.astype(jnp.float32)
    normed = (widened * lax.rsqrt(lax.optimization_barrier(jnp.mean(widened * widened, axis=1, keepdims=True)) + 1e-06) * norm_gain).astype(jnp.bfloat16)
    flat_ids = expert_ids.reshape(-1)
    flat_weights = route_weights.reshape(-1)
    owners = jnp.arange(LENGTH * TOPK, dtype=jnp.int32) // TOPK
    most_rows = LENGTH // ROWS * CAP
    slice_width = FF // N_TP

    def expert_step(gathered, expert):
        matches = flat_ids == expert
        chosen = jnp.nonzero(matches, size=most_rows, fill_value=0)[0].astype(jnp.int32)
        filled = (jnp.arange(most_rows, dtype=jnp.int32) < jnp.sum(matches.astype(jnp.int32))).astype(jnp.float32)
        targets = owners[chosen]
        inputs = normed[targets]
        gate_part = jnp.dot(inputs, gate_weight[expert], preferred_element_type=jnp.float32)
        up_part = jnp.dot(inputs, up_weight[expert], preferred_element_type=jnp.float32)
        inner_rows = (jax.nn.silu(gate_part) * up_part).astype(jnp.bfloat16)
        pieces = jnp.einsum('mtf,tfd->mtd', inner_rows.reshape(most_rows, N_TP, slice_width).astype(jnp.float32), down_weight[expert].reshape(N_TP, slice_width, D).astype(jnp.float32))
        pieces = lax.optimization_barrier(pieces.astype(jnp.bfloat16)).astype(jnp.float32)
        result = lax.optimization_barrier(lax.optimization_barrier(jnp.sum(pieces, axis=1)).astype(jnp.bfloat16)).astype(jnp.float32)
        scaled = result * (flat_weights[chosen] * filled)[:, None]
        return (gathered.at[targets].add(scaled), None)
    moe_sum, leftover = lax.scan(expert_step, jnp.zeros((LENGTH, D), jnp.float32), jnp.arange(EXPERTS, dtype=jnp.int32))
    return (updated.astype(jnp.float32) + moe_sum).astype(jnp.bfloat16)
```

```python
import functools
import math

import jax
import jax.numpy as jnp
from jax import lax
from jax.experimental import pallas as pl
from jax.experimental.pallas import tpu as pltpu
from jax.sharding import PartitionSpec as P

LANES = 128
OWNERS_PER_TILE = 4


def attention_kernel(
    part_ref, lam_ref, gain_ref, rows_ref, out_ref, stack_ref, acc_ref, top_ref, *, sub, key_rows, parts, scale
):
    tile = pl.program_id(0)
    tile_rows = OWNERS_PER_TILE * sub
    span = tile_rows * parts
    width = rows_ref.shape[2]
    half = width // 2
    query_rows = key_rows // parts
    tiles_per_source = key_rows // span

    source = tile // tiles_per_source
    start = pl.multiple_of((tile % tiles_per_source) * tile_rows, tile_rows)
    query = rows_ref[source, pl.ds(start, tile_rows), :]
    low = lax.broadcasted_iota(jnp.int32, (tile_rows, width), 1) < half
    nothing = jnp.zeros_like(query)
    stack_ref[0:tile_rows, :] = jnp.where(low, query, nothing)
    stack_ref[tile_rows:, :] = jnp.where(low, nothing, query)
    top_ref[...] = jnp.full_like(top_ref, -1e30)
    acc_ref[...] = jnp.zeros_like(acc_ref)
    ones = jnp.ones((span, LANES), jnp.bfloat16)

    def one_tile(index, diagonal):
        owner = index // tiles_per_source
        offset = pl.multiple_of((index % tiles_per_source) * span, span)
        keys = rows_ref[owner, pl.ds(query_rows + offset, span), :]
        values = rows_ref[owner, pl.ds(query_rows + key_rows + offset, span), :]
        scores = (
            lax.dot_general(
                stack_ref[...], keys, (((1,), (1,)), ((), ())), preferred_element_type=jnp.float32
            )
            * scale
        )
        if diagonal:
            row = lax.broadcasted_iota(jnp.int32, (tile_rows, LANES), 0)
            place = row + part_ref[0] * sub
            for step in range(1, OWNERS_PER_TILE):
                place = place + jnp.where(row >= step * sub, (parts - 1) * sub, 0)
            gap = place - lax.broadcasted_iota(jnp.int32, (tile_rows, LANES), 1)
            gap = jnp.concatenate([gap, gap], axis=0)
            scores = jnp.concatenate(
                [
                    jnp.where(gap >= first, scores[:, first : first + LANES], -jnp.inf)
                    for first in range(0, span, LANES)
                ],
                axis=1,
            )
        before = top_ref[...]
        after = jnp.maximum(before, jnp.max(scores, axis=1, keepdims=True))
        decay = jnp.exp(before - after)
        weights = jnp.exp(scores - after[:, :1])
        top_ref[...] = after
        acc_ref[...] = acc_ref[...] * decay[:, :1] + jnp.dot(
            weights.astype(jnp.bfloat16),
            jnp.concatenate([values, ones], axis=1),
            preferred_element_type=jnp.float32,
        )

    one_tile(tile, True)

    @pl.loop(0, tile)
    def _(index):
        one_tile(index, False)

    first = acc_ref[0:tile_rows, :]
    second = acc_ref[tile_rows:, :]
    mixed = (
        first[:, :width] / first[:, width : width + 1]
        - lam_ref[0] * second[:, :width] / second[:, width : width + 1]
    )
    scaled = mixed * lax.rsqrt(jnp.mean(mixed * mixed, axis=1, keepdims=True) + 1e-06)
    out_ref[...] = (scaled * gain_ref[...]).astype(out_ref.dtype)


def attention(part, lam, gain, arrived, sub, key_rows, parts, scale):
    sources, _, width = arrived.shape
    tile_rows = OWNERS_PER_TILE * sub
    total_rows = sources * key_rows // parts
    pairs = total_rows * sources * key_rows
    return pl.pallas_call(
        functools.partial(attention_kernel, sub=sub, key_rows=key_rows, parts=parts, scale=scale),
        grid=(total_rows // tile_rows,),
        out_shape=jax.ShapeDtypeStruct((total_rows, width), jnp.bfloat16),
        in_specs=[
            pl.BlockSpec(memory_space=pltpu.SMEM),
            pl.BlockSpec(memory_space=pltpu.SMEM),
            pl.BlockSpec((1, width), lambda i: (0, 0)),
            pl.BlockSpec(memory_space=pltpu.VMEM),
        ],
        out_specs=pl.BlockSpec((tile_rows, width), lambda i: (i, 0)),
        scratch_shapes=[
            pltpu.VMEM((2 * tile_rows, width), jnp.bfloat16),
            pltpu.VMEM((2 * tile_rows, width + LANES), jnp.float32),
            pltpu.VMEM((2 * tile_rows, LANES), jnp.float32),
        ],
        compiler_params=pltpu.CompilerParams(vmem_limit_bytes=32 * 1024 * 1024),
        cost_estimate=pl.CostEstimate(
            flops=8 * pairs * width, bytes_accessed=2 * arrived.size, transcendentals=pairs
        ),
        name="attention",
    )(part, lam, gain, arrived)


def project_kernel(heads_ref, weight_ref, residual_ref, gain_ref, routes_ref, updated_ref, normed_ref, acc_ref, *, parts):
    step = pl.program_id(0)
    sub, width = heads_ref.shape[2:]
    held = heads_ref.shape[0] // parts
    left = jnp.concatenate(
        [
            jnp.concatenate([heads_ref[part * held + head, 0] for head in range(held)], axis=1)
            for part in range(parts)
        ],
        axis=0,
    )
    product = jnp.dot(left, weight_ref[...], preferred_element_type=jnp.float32)

    @pl.when(step == 0)
    def _():
        acc_ref[...] = residual_ref[...].astype(jnp.float32) + product

    @pl.when(step > 0)
    def _():
        acc_ref[...] += product

    @pl.when(step == pl.num_programs(0) - 1)
    def _():
        updated = acc_ref[...].astype(jnp.bfloat16)
        updated_ref[...] = updated
        wide = updated.astype(jnp.float32)
        scaled = wide * lax.rsqrt(jnp.mean(wide * wide, axis=1, keepdims=True) + 1e-06)
        model = wide.shape[1]
        normed_ref[:, :model] = (scaled * gain_ref[...]).astype(jnp.bfloat16)
        normed_ref[:, model:] = routes_ref[...]


def project(heads, out_weight, residual, gain, routes, parts):
    sources, columns, sub, width = heads.shape
    rows, model = residual.shape
    depth = sources // parts * width
    return pl.pallas_call(
        functools.partial(project_kernel, parts=parts),
        grid=(columns,),
        out_shape=(
            jax.ShapeDtypeStruct((rows, model), jnp.bfloat16),
            jax.ShapeDtypeStruct((rows, model + LANES), jnp.bfloat16),
        ),
        in_specs=[
            pl.BlockSpec((sources, 1, sub, width), lambda i: (0, i, 0, 0)),
            pl.BlockSpec((depth, model), lambda i: (i, 0)),
            pl.BlockSpec((rows, model), lambda i: (0, 0)),
            pl.BlockSpec((1, model), lambda i: (0, 0)),
            pl.BlockSpec((rows, LANES), lambda i: (0, 0)),
        ],
        out_specs=(
            pl.BlockSpec((rows, model), lambda i: (0, 0)),
            pl.BlockSpec((rows, model + LANES), lambda i: (0, 0)),
        ),
        scratch_shapes=[pltpu.VMEM((rows, model), jnp.float32)],
        compiler_params=pltpu.CompilerParams(vmem_limit_bytes=24 * 1024 * 1024),
        cost_estimate=pl.CostEstimate(
            flops=2 * rows * model * columns * depth, bytes_accessed=2 * out_weight.size, transcendentals=0
        ),
        name="project",
    )(heads, out_weight, residual, gain, routes)


def expert_kernel(*refs, blocks, experts):
    first_ref = refs[0]
    block_refs = refs[1 : 1 + blocks]
    gate_a, up_a, down_a, gate_b, up_b, down_b = refs[1 + blocks : 7 + blocks]
    out_refs = refs[7 + blocks : 7 + 2 * blocks]
    rows_ref, acc_ref = refs[7 + 2 * blocks :]
    expert = pl.program_id(0)
    model = rows_ref.shape[1] - LANES

    @pl.when(expert == 0)
    def _():
        place = 0
        for ref in block_refs:
            rows_ref[place : place + ref.shape[0], :] = ref[...]
            place += ref.shape[0]

    routes = rows_ref[:, model:].astype(jnp.float32)
    lane = lax.broadcasted_iota(jnp.int32, routes.shape, 1)
    mine = first_ref[0] + expert
    share = jnp.sum(
        jnp.where((lane == mine) | (lane == mine + experts), routes, 0.0), axis=1, keepdims=True
    )
    rows = rows_ref[:, :model]
    product = None
    for gate_ref, up_ref, down_ref in ((gate_a, up_a, down_a), (gate_b, up_b, down_b)):
        gate = jnp.dot(rows, gate_ref[0], preferred_element_type=jnp.float32)
        up = jnp.dot(rows, up_ref[0], preferred_element_type=jnp.float32)
        inner = (gate / (1.0 + jnp.exp(-gate)) * up * share).astype(jnp.bfloat16)
        term = jnp.dot(inner, down_ref[0], preferred_element_type=jnp.float32)
        product = term if product is None else product + term

    @pl.when(expert == 0)
    def _():
        acc_ref[...] = product

    @pl.when(expert > 0)
    def _():
        acc_ref[...] += product

    @pl.when(expert == pl.num_programs(0) - 1)
    def _():
        place = 0
        for ref in out_refs:
            ref[...] = acc_ref[place : place + ref.shape[0], :].astype(jnp.bfloat16)
            place += ref.shape[0]


def expert_pass(first, blocks, weights, experts):
    held, model, hidden = weights[0].shape
    total = sum(block.shape[0] for block in blocks)
    whole = [pl.BlockSpec(block.shape, lambda i: (0, 0)) for block in blocks]
    wide = pl.BlockSpec((1, model, hidden), lambda i: (i, 0, 0))
    tall = pl.BlockSpec((1, hidden, model), lambda i: (i, 0, 0))
    return pl.pallas_call(
        functools.partial(expert_kernel, blocks=len(blocks), experts=experts),
        grid=(held,),
        out_shape=tuple(
            jax.ShapeDtypeStruct((block.shape[0], model), jnp.bfloat16) for block in blocks
        ),
        in_specs=[pl.BlockSpec(memory_space=pltpu.SMEM), *whole, wide, wide, tall, wide, wide, tall],
        out_specs=tuple(
            pl.BlockSpec((block.shape[0], model), lambda i: (0, 0)) for block in blocks
        ),
        scratch_shapes=[
            pltpu.VMEM((total, model + LANES), jnp.bfloat16),
            pltpu.VMEM((total, model), jnp.float32),
        ],
        compiler_params=pltpu.CompilerParams(vmem_limit_bytes=40 * 1024 * 1024),
        cost_estimate=pl.CostEstimate(
            flops=12 * held * total * model * hidden,
            bytes_accessed=12 * held * model * hidden,
            transcendentals=2 * held * total * hidden,
        ),
        name="experts",
    )(first, *blocks, *weights)


def balanced(
    queries,
    key_pairs,
    head_values,
    lambdas,
    head_gain,
    out_weight,
    residual,
    norm_gain,
    expert_ids,
    route_weights,
    gate_weight,
    up_weight,
    down_weight,
):
    tokens, heads, width = queries.shape
    rows, model = residual.shape
    sp_count, tp_count = lax.axis_size("sp"), lax.axis_size("tp")
    sp_index = lax.axis_index("sp")
    parts = sp_count // heads
    sub = rows // parts
    held = gate_weight.shape[0]
    experts = held * sp_count

    swap = [(i, i ^ 1) for i in range(tp_count)]
    mine = (gate_weight, up_weight, down_weight)
    other = tuple(lax.ppermute(w, "tp", swap) for w in mine)

    split = jnp.transpose(
        queries.reshape(tp_count, parts, sub, heads, width), (1, 3, 0, 2, 4)
    ).reshape(sp_count, tokens // parts, width)
    keys = jnp.tile(jnp.transpose(key_pairs, (1, 0, 2)), (parts, 1, 1))
    values = jnp.tile(jnp.transpose(head_values, (1, 0, 2)), (parts, 1, 1))
    arrived = lax.all_to_all(
        jnp.concatenate([split, keys, values], axis=1), "sp", split_axis=0, concat_axis=0, tiled=True
    )
    attended = attention(
        (sp_index // heads).reshape(1),
        lax.dynamic_slice_in_dim(lambdas, sp_index % heads, 1),
        head_gain.reshape(1, -1),
        arrived,
        sub,
        tokens,
        parts,
        (width // 2) ** (-0.5),
    )
    regrouped = lax.all_to_all(
        attended.reshape(sp_count * tp_count, sub, width),
        ("sp", "tp"),
        split_axis=0,
        concat_axis=0,
        tiled=True,
    ).reshape(sp_count, tp_count, sub, width)

    share = jnp.sum(
        jnp.where(
            expert_ids[:, :, None] == jnp.arange(experts, dtype=jnp.int32),
            route_weights[:, :, None],
            0.0,
        ),
        axis=1,
    )
    coarse = lax.reduce_precision(share, 8, 7)
    routes = jnp.concatenate(
        [coarse, share - coarse, jnp.zeros((rows, LANES - 2 * experts), jnp.float32)], axis=1
    ).astype(jnp.bfloat16)
    updated, normed = project(
        regrouped, out_weight, residual, norm_gain.reshape(1, -1), routes, parts
    )

    across_x = [(i, i ^ 1) for i in range(sp_count)]
    across_y = [(i, i ^ 2) for i in range(sp_count)]

    def turned(array, steps):
        return lax.ppermute(
            array, "tp", [(i, (i + 2 * steps) % tp_count) for i in range(tp_count)]
        )

    layers = tp_count // 2
    cut = rows // 2
    sources = [normed] + [turned(normed, -k) for k in range(1, layers)]
    first = (sp_index * held).reshape(1)
    weights = (*mine, *other)
    reduced = []
    for block in sources:
        by_x = lax.ppermute(block, "sp", across_x)
        by_y = lax.ppermute(block, "sp", across_y)
        far_low = lax.ppermute(by_x[:cut], "sp", across_y)
        far_high = lax.ppermute(by_y[cut:], "sp", across_x)
        own, to_x, to_y, to_low, to_high = expert_pass(
            first, (block, by_x, by_y, far_low, far_high), weights, experts
        )
        add_low = lax.ppermute(to_low, "sp", across_y)
        add_high = lax.ppermute(to_high, "sp", across_x)
        to_x = jnp.concatenate(
            [(to_x[:cut].astype(jnp.float32) + add_low.astype(jnp.float32)).astype(jnp.bfloat16), to_x[cut:]]
        )
        to_y = jnp.concatenate(
            [to_y[:cut], (to_y[cut:].astype(jnp.float32) + add_high.astype(jnp.float32)).astype(jnp.bfloat16)]
        )
        from_x = lax.ppermute(to_x, "sp", across_x)
        from_y = lax.ppermute(to_y, "sp", across_y)
        reduced.append(
            own.astype(jnp.float32) + from_x.astype(jnp.float32) + from_y.astype(jnp.float32)
        )
    total = updated.astype(jnp.float32) + reduced[0]
    for k in range(1, layers):
        total = total + turned(reduced[k].astype(jnp.bfloat16), k).astype(jnp.float32)
    return total.astype(jnp.bfloat16)


def shards(
    queries,
    key_pairs,
    head_values,
    lambdas,
    head_gain,
    out_weight,
    residual,
    norm_gain,
    expert_ids,
    route_weights,
    gate_weight,
    up_weight,
    down_weight,
):
    tokens_here, heads_here, pair_width = queries.shape
    half_width = pair_width // 2
    value_width = head_values.shape[2]
    score_scale = half_width ** (-0.5)
    query_pos = lax.axis_index("sp") * tokens_here + jnp.arange(tokens_here, dtype=jnp.int32)
    split_queries = queries.reshape(tokens_here, heads_here, 2, half_width)
    start_state = (
        jnp.full((2, heads_here, tokens_here), -1e30, jnp.float32),
        jnp.zeros((2, heads_here, tokens_here), jnp.float32),
        jnp.zeros((2, heads_here, tokens_here, value_width), jnp.float32),
    )
    key_piece = lax.all_gather(key_pairs, "sp", axis=0, tiled=True)
    value_piece = lax.all_gather(head_values, "sp", axis=0, tiled=True)
    span_rows = key_piece.shape[0]
    width_rows = math.gcd(span_rows, 512)

    def block_step(block_index, state):
        running_max, totals, summed = state
        offset = block_index * width_rows
        key_block = lax.dynamic_slice_in_dim(key_piece, offset, width_rows, 0).reshape(
            width_rows, heads_here, 2, half_width
        )
        value_block = lax.dynamic_slice_in_dim(value_piece, offset, width_rows, 0)
        key_pos = offset + jnp.arange(width_rows, dtype=jnp.int32)
        allowed = key_pos[None, :] <= query_pos[:, None]
        scores = (
            jnp.einsum(
                "qhcd,khcd->chqk", split_queries, key_block, preferred_element_type=jnp.float32
            )
            * score_scale
        )
        scores = jnp.where(allowed[None, None], scores, -jnp.inf)
        fresh_max = jnp.maximum(running_max, jnp.max(scores, axis=3))
        decay = jnp.exp(running_max - fresh_max)
        weights = jnp.exp(scores - fresh_max[..., None])
        totals = totals * decay + jnp.sum(weights, axis=3)
        summed = summed * decay[..., None] + jnp.einsum(
            "chqk,khv->chqv",
            weights.astype(jnp.bfloat16),
            value_block,
            preferred_element_type=jnp.float32,
        )
        return (fresh_max, totals, summed)

    def through(state):
        return lax.fori_loop(0, span_rows // width_rows, block_step, state)

    def untouched(state):
        return state

    running_max, totals, summed = lax.cond(
        jnp.int32(0) <= query_pos[-1], through, untouched, start_state
    )
    mixed = (
        summed[0] / totals[0][..., None] - lambdas[:, None, None] * summed[1] / totals[1][..., None]
    )
    normed_heads = (
        mixed * lax.rsqrt(jnp.mean(mixed * mixed, axis=2, keepdims=True) + 1e-06) * head_gain
    )
    attended = (
        jnp.transpose(normed_heads, (1, 0, 2))
        .reshape(tokens_here, heads_here * value_width)
        .astype(jnp.bfloat16)
    )
    rows_here = residual.shape[0]
    regrouped = lax.all_to_all(attended, "tp", split_axis=0, concat_axis=1, tiled=True)
    projected = jnp.dot(regrouped, out_weight, preferred_element_type=jnp.float32)
    updated = (residual.astype(jnp.float32) + projected).astype(jnp.bfloat16)
    widened = updated.astype(jnp.float32)
    normed = (
        widened * lax.rsqrt(jnp.mean(widened * widened, axis=1, keepdims=True) + 1e-06) * norm_gain
    ).astype(jnp.bfloat16)
    route_count = expert_ids.shape[1]
    local_experts = gate_weight.shape[0]
    sp_count = lax.axis_size("sp")
    expert_count = local_experts * sp_count
    capacity = max(2, 4 * rows_here * route_count // (3 * expert_count))
    model_width = normed.shape[1]
    flat_ids = expert_ids.reshape(-1)
    indicator = (flat_ids[:, None] == jnp.arange(expert_count, dtype=jnp.int32)[None, :]).astype(
        jnp.int32
    )
    ranking = jnp.sum(jnp.cumsum(indicator, axis=0) * indicator, axis=1) - 1
    slots = flat_ids * capacity + ranking
    sources = jnp.arange(rows_here * route_count, dtype=jnp.int32) // route_count
    outgoing = (
        jnp.zeros((expert_count * capacity, model_width), jnp.bfloat16)
        .at[slots]
        .set(normed[sources])
    )
    arrived = lax.all_to_all(
        outgoing.reshape(sp_count, local_experts, capacity, model_width),
        "sp",
        split_axis=0,
        concat_axis=0,
        tiled=True,
    )
    piece_rows = lax.all_gather(arrived[None], "tp", axis=0, tiled=True)
    gate_part = jnp.einsum(
        "tsecd,edf->tsecf", piece_rows, gate_weight, preferred_element_type=jnp.float32
    )
    up_part = jnp.einsum(
        "tsecd,edf->tsecf", piece_rows, up_weight, preferred_element_type=jnp.float32
    )
    inner_rows = (jax.nn.silu(gate_part) * up_part).astype(jnp.bfloat16)
    partial_value = jnp.einsum(
        "tsecf,efd->tsecd", inner_rows, down_weight, preferred_element_type=jnp.float32
    )
    reduced = lax.psum_scatter(
        partial_value.astype(jnp.bfloat16), "tp", scatter_dimension=0, tiled=True
    )
    returned = lax.all_to_all(reduced[0], "sp", split_axis=0, concat_axis=0, tiled=True)
    picked = (
        returned.reshape(expert_count * capacity, model_width)[slots]
        .astype(jnp.float32)
        .reshape(rows_here, route_count, model_width)
    )
    moe_sum = jnp.sum(picked * route_weights[:, :, None], axis=1)
    return (updated.astype(jnp.float32) + moe_sum).astype(jnp.bfloat16)


def fits_balanced(queries, residual, expert_ids, gate_weight, sp_count, tp_count):
    tokens, heads, width = queries.shape
    rows = residual.shape[0]
    held = gate_weight.shape[0]
    if sp_count != 4 or tp_count % 2 or sp_count % heads or width != LANES:
        return False
    sub = rows // (sp_count // heads)
    span = OWNERS_PER_TILE * rows
    capacity = 4 * rows * expert_ids.shape[1] // (3 * held * sp_count)
    return (
        sub % 16 == 0
        and rows % 32 == 0
        and tokens % span == 0
        and span % LANES == 0
        and 2 * held * sp_count <= LANES
        and 2 * held * capacity >= rows
    )


def layer(*args):
    queries, residual, expert_ids, gate_weight = args[0], args[6], args[8], args[10]
    chosen = fits_balanced(
        queries, residual, expert_ids, gate_weight, lax.axis_size("sp"), lax.axis_size("tp")
    )
    return (balanced if chosen else shards)(*args)


def solution(mesh):
    placed = (
        P("sp", "tp", None),
        P("sp", "tp", None),
        P("sp", "tp", None),
        P("tp"),
        P(),
        P(),
        P(("sp", "tp"), None),
        P(),
        P(("sp", "tp"), None),
        P(("sp", "tp"), None),
        P("sp", None, "tp"),
        P("sp", None, "tp"),
        P("sp", "tp", None),
    )
    return jax.shard_map(
        layer, mesh=mesh, in_specs=placed, out_specs=P(("sp", "tp"), None), check_vma=False
    )
```

```python
import functools
import math

import jax
import jax.numpy as jnp
from jax import lax
from jax.experimental import pallas as pl
from jax.experimental.pallas import tpu as pltpu
from jax.sharding import PartitionSpec as P

LANES = 128
OWNERS_PER_TILE = 4


def attention_kernel(
    part_ref,
    lam_ref,
    gain_ref,
    rows_ref,
    out_ref,
    stack_ref,
    score_ref,
    acc_ref,
    top_ref,
    *,
    sub,
    key_rows,
    parts,
    scale,
):
    tile = pl.program_id(0)
    exact = math.frexp(scale)[0] == 0.5
    tile_rows = OWNERS_PER_TILE * sub
    span = tile_rows * parts
    width = rows_ref.shape[2]
    half = width // 2
    query_rows = key_rows // parts
    tiles_per_source = key_rows // span

    source = tile // tiles_per_source
    start = pl.multiple_of((tile % tiles_per_source) * tile_rows, tile_rows)
    query = rows_ref[source, pl.ds(start, tile_rows), :]
    if exact:
        query = (query.astype(jnp.float32) * scale).astype(jnp.bfloat16)
    low = lax.broadcasted_iota(jnp.int32, (tile_rows, width), 1) < half
    nothing = jnp.zeros_like(query)
    stack_ref[0:tile_rows, :] = jnp.where(low, query, nothing)
    stack_ref[tile_rows:, :] = jnp.where(low, nothing, query)
    top_ref[...] = jnp.full_like(top_ref, -1e30)
    acc_ref[...] = jnp.zeros_like(acc_ref)
    ones = jnp.ones((span, LANES), jnp.bfloat16)

    def place_of(index, base):
        offset = pl.multiple_of((index % tiles_per_source) * span, span)
        return index // tiles_per_source, pl.ds(base + offset, span)

    def score(index):
        owner, place = place_of(index, query_rows)
        scores = lax.dot_general(
            stack_ref[...],
            rows_ref[owner, place, :],
            (((1,), (1,)), ((), ())),
            preferred_element_type=jnp.float32,
        )
        return scores if exact else scores * scale

    def absorb(index, scores):
        owner, place = place_of(index, query_rows + key_rows)
        before = top_ref[...]
        after = jnp.maximum(before, jnp.max(scores, axis=1, keepdims=True))
        decay = jnp.exp(before - after)
        weights = jnp.exp(scores - jnp.concatenate([after] * (span // LANES), axis=1))
        top_ref[...] = after
        acc_ref[...] = acc_ref[...] * jnp.concatenate(
            [decay] * (1 + width // LANES), axis=1
        ) + jnp.dot(
            weights.astype(jnp.bfloat16),
            jnp.concatenate([rows_ref[owner, place, :], ones], axis=1),
            preferred_element_type=jnp.float32,
        )

    score_ref[0] = score(0)

    @pl.loop(0, tile)
    def _(index):
        score_ref[(index + 1) % 2] = score(index + 1)
        absorb(index, score_ref[index % 2])

    scores = score_ref[tile % 2]
    row = lax.broadcasted_iota(jnp.int32, (tile_rows, LANES), 0)
    place = row + part_ref[0] * sub
    for step in range(1, OWNERS_PER_TILE):
        place = place + jnp.where(row >= step * sub, (parts - 1) * sub, 0)
    gap = place - lax.broadcasted_iota(jnp.int32, (tile_rows, LANES), 1)
    gap = jnp.concatenate([gap, gap], axis=0)
    absorb(
        tile,
        jnp.concatenate(
            [
                jnp.where(gap >= first, scores[:, first : first + LANES], -jnp.inf)
                for first in range(0, span, LANES)
            ],
            axis=1,
        ),
    )

    first = acc_ref[0:tile_rows, :]
    second = acc_ref[tile_rows:, :]
    mixed = first[:, :width] / first[:, width:] - lam_ref[0] * second[:, :width] / second[:, width:]
    scaled = mixed * lax.rsqrt(jnp.mean(mixed * mixed, axis=1, keepdims=True) + 1e-06)
    out_ref[...] = (scaled * gain_ref[...]).astype(out_ref.dtype)


def attention(part, lam, gain, arrived, sub, key_rows, parts, scale):
    sources, _, width = arrived.shape
    tile_rows = OWNERS_PER_TILE * sub
    total_rows = sources * key_rows // parts
    pairs = total_rows * sources * key_rows
    return pl.pallas_call(
        functools.partial(
            attention_kernel, sub=sub, key_rows=key_rows, parts=parts, scale=scale
        ),
        grid=(total_rows // tile_rows,),
        out_shape=jax.ShapeDtypeStruct((total_rows, width), jnp.bfloat16),
        in_specs=[
            pl.BlockSpec(memory_space=pltpu.SMEM),
            pl.BlockSpec(memory_space=pltpu.SMEM),
            pl.BlockSpec((1, width), lambda i: (0, 0)),
            pl.BlockSpec(memory_space=pltpu.VMEM),
        ],
        out_specs=pl.BlockSpec((tile_rows, width), lambda i: (i, 0)),
        scratch_shapes=[
            pltpu.VMEM((2 * tile_rows, width), jnp.bfloat16),
            pltpu.VMEM((2, 2 * tile_rows, tile_rows * parts), jnp.float32),
            pltpu.VMEM((2 * tile_rows, width + LANES), jnp.float32),
            pltpu.VMEM((2 * tile_rows, LANES), jnp.float32),
        ],
        compiler_params=pltpu.CompilerParams(vmem_limit_bytes=12 * 1024 * 1024),
        cost_estimate=pl.CostEstimate(
            flops=8 * pairs * width, bytes_accessed=2 * arrived.size, transcendentals=pairs
        ),
        name="attention",
    )(part, lam, gain, arrived)


def project_kernel(heads_ref, weight_ref, residual_ref, gain_ref, routes_ref, updated_ref, normed_ref, acc_ref, *, parts):
    step = pl.program_id(0)
    held = heads_ref.shape[0] // parts
    left = jnp.concatenate(
        [
            jnp.concatenate([heads_ref[part * held + head, 0] for head in range(held)], axis=1)
            for part in range(parts)
        ],
        axis=0,
    )
    product = jnp.dot(left, weight_ref[...], preferred_element_type=jnp.float32)

    @pl.when(step == 0)
    def _():
        acc_ref[...] = residual_ref[...].astype(jnp.float32) + product

    @pl.when(step > 0)
    def _():
        acc_ref[...] += product

    @pl.when(step == pl.num_programs(0) - 1)
    def _():
        updated = acc_ref[...].astype(jnp.bfloat16)
        updated_ref[...] = updated
        wide = updated.astype(jnp.float32)
        scaled = wide * lax.rsqrt(jnp.mean(wide * wide, axis=1, keepdims=True) + 1e-06)
        model = wide.shape[1]
        normed_ref[:, :model] = (scaled * gain_ref[...]).astype(jnp.bfloat16)
        normed_ref[:, model:] = routes_ref[...]


def project(heads, out_weight, residual, gain, routes, parts):
    sources, columns, sub, width = heads.shape
    rows, model = residual.shape
    depth = sources // parts * width
    return pl.pallas_call(
        functools.partial(project_kernel, parts=parts),
        grid=(columns,),
        out_shape=(
            jax.ShapeDtypeStruct((rows, model), jnp.bfloat16),
            jax.ShapeDtypeStruct((rows, model + LANES), jnp.bfloat16),
        ),
        in_specs=[
            pl.BlockSpec((sources, 1, sub, width), lambda i: (0, i, 0, 0)),
            pl.BlockSpec((depth, model), lambda i: (i, 0)),
            pl.BlockSpec((rows, model), lambda i: (0, 0)),
            pl.BlockSpec((1, model), lambda i: (0, 0)),
            pl.BlockSpec((rows, LANES), lambda i: (0, 0)),
        ],
        out_specs=(
            pl.BlockSpec((rows, model), lambda i: (0, 0)),
            pl.BlockSpec((rows, model + LANES), lambda i: (0, 0)),
        ),
        scratch_shapes=[pltpu.VMEM((rows, model), jnp.float32)],
        compiler_params=pltpu.CompilerParams(vmem_limit_bytes=48 * 1024 * 1024),
        cost_estimate=pl.CostEstimate(
            flops=2 * rows * model * columns * depth, bytes_accessed=2 * out_weight.size, transcendentals=0
        ),
        name="project",
    )(heads, out_weight, residual, gain, routes)


def choose_kernel(place_ref, block_ref, chosen_ref, *out_refs, held, experts, capacity):
    model = block_ref.shape[1] - LANES
    slots = len(out_refs) * held * capacity
    source = lax.broadcasted_iota(jnp.int32, (LANES, slots), 0)
    slot = lax.broadcasted_iota(jnp.int32, (LANES, slots), 1)
    wanted = 0 * slot
    for column in range(len(out_refs)):
        for expert in range(held):
            first = (column * held + expert) * capacity
            name = jnp.bitwise_xor(place_ref[0], column) * held + expert
            inside = (slot >= first) & (slot < first + capacity)
            wanted = jnp.where(inside, 2 * experts + name, wanted)
    table = jnp.where(source == wanted, 1.0, 0.0).astype(jnp.bfloat16)
    ranks = jnp.dot(block_ref[:, model:], table, preferred_element_type=jnp.float32)
    lane = lax.broadcasted_iota(jnp.int32, ranks.shape, 1)
    order = lax.rem(lane, capacity).astype(jnp.float32)
    chosen = jnp.where(ranks == order, 1.0, 0.0).astype(jnp.bfloat16)
    chosen_ref[...] = chosen
    rows = lax.dot_general(
        chosen, block_ref[...], (((0,), (0,)), ((), ())), preferred_element_type=jnp.float32
    ).astype(jnp.bfloat16)
    for column, out_ref in enumerate(out_refs):
        out_ref[...] = rows[column * held * capacity : (column + 1) * held * capacity]


def choose(place, block, columns, held, experts, capacity):
    rows, width = block.shape
    slots = held * capacity
    whole = pl.BlockSpec(memory_space=pltpu.VMEM)
    return pl.pallas_call(
        functools.partial(choose_kernel, held=held, experts=experts, capacity=capacity),
        out_shape=(
            jax.ShapeDtypeStruct((rows, columns * slots), jnp.bfloat16),
            *(jax.ShapeDtypeStruct((slots, width), jnp.bfloat16) for _ in range(columns)),
        ),
        in_specs=[pl.BlockSpec(memory_space=pltpu.SMEM), whole],
        out_specs=(whole,) * (columns + 1),
        compiler_params=pltpu.CompilerParams(vmem_limit_bytes=16 * 1024 * 1024),
        cost_estimate=pl.CostEstimate(
            flops=2 * rows * width * columns * slots, bytes_accessed=4 * rows * width, transcendentals=0
        ),
        name="choose",
    )(place, block)


def merge_kernel(chosen_ref, *refs):
    out_ref, kept_ref = refs[-2:]
    slots = refs[0].shape[0]
    for column, ref in enumerate(refs[:-2]):
        kept_ref[column * slots : (column + 1) * slots, :] = ref[...]
    total = jnp.dot(chosen_ref[...], kept_ref[...], preferred_element_type=jnp.float32)
    out_ref[...] = total.astype(out_ref.dtype)


def merge(chosen, parts):
    rows = chosen.shape[0]
    model = parts[0].shape[1]
    whole = pl.BlockSpec(memory_space=pltpu.VMEM)
    return pl.pallas_call(
        merge_kernel,
        out_shape=jax.ShapeDtypeStruct((rows, model), jnp.bfloat16),
        in_specs=[whole] * (1 + len(parts)),
        out_specs=whole,
        scratch_shapes=[pltpu.VMEM((chosen.shape[1], model), jnp.bfloat16)],
        compiler_params=pltpu.CompilerParams(vmem_limit_bytes=16 * 1024 * 1024),
        cost_estimate=pl.CostEstimate(
            flops=2 * rows * chosen.shape[1] * model, bytes_accessed=4 * rows * model, transcendentals=0
        ),
        name="merge",
    )(chosen, *parts)


def expert_kernel(*refs, blocks, experts):
    first_ref = refs[0]
    block_refs = refs[1 : 1 + blocks]
    weight_refs = refs[1 + blocks : 7 + blocks]
    out_refs = refs[7 + blocks : 7 + 2 * blocks]
    kept_refs = refs[7 + 2 * blocks : 13 + 2 * blocks]
    rows_ref, sems = refs[13 + 2 * blocks :]
    model = rows_ref.shape[2] - LANES
    held = kept_refs[0].shape[0]
    capacity = block_refs[0].shape[0] // held
    sets = ((0, 1, 2), (3, 4, 5))

    def copy(index, expert):
        return pltpu.make_async_copy(
            weight_refs[index].at[expert], kept_refs[index].at[expert], sems.at[index, expert]
        )

    for expert in range(held):
        for indices in sets:
            for index in indices:
                copy(index, expert).start()

    for expert in range(held):
        for number, ref in enumerate(block_refs):
            rows_ref[expert, number * capacity : (number + 1) * capacity, :] = ref[
                expert * capacity : (expert + 1) * capacity, :
            ]

    for expert in range(held):
        routes = rows_ref[expert, :, model:].astype(jnp.float32)
        lane = lax.broadcasted_iota(jnp.int32, routes.shape, 1)
        mine = first_ref[0] + expert
        share = jnp.sum(
            jnp.where((lane == mine) | (lane == mine + experts), routes, 0.0), axis=1, keepdims=True
        )
        rows = rows_ref[expert, :, :model]
        total = None
        for indices in sets:
            parts = []
            for index in indices[:2]:
                copy(index, expert).wait()
                parts.append(
                    jnp.dot(rows, kept_refs[index][expert], preferred_element_type=jnp.float32)
                )
            gate, up = parts
            inner = (gate / (1.0 + jnp.exp(-gate)) * up * share).astype(jnp.bfloat16)
            copy(indices[2], expert).wait()
            term = jnp.dot(inner, kept_refs[indices[2]][expert], preferred_element_type=jnp.float32)
            total = term if total is None else total + term
        total = total.astype(jnp.bfloat16)
        for number, ref in enumerate(out_refs):
            ref[expert * capacity : (expert + 1) * capacity, :] = total[
                number * capacity : (number + 1) * capacity
            ]


def expert_pass(first, blocks, weights, experts):
    held, model, hidden = weights[0].shape
    slots = blocks[0].shape[0]
    total = len(blocks) * slots
    whole = pl.BlockSpec(memory_space=pltpu.VMEM)
    return pl.pallas_call(
        functools.partial(expert_kernel, blocks=len(blocks), experts=experts),
        out_shape=tuple(jax.ShapeDtypeStruct((slots, model), jnp.bfloat16) for _ in blocks),
        in_specs=[pl.BlockSpec(memory_space=pltpu.SMEM)]
        + [whole] * len(blocks)
        + [pl.BlockSpec(memory_space=pl.ANY)] * len(weights),
        out_specs=(whole,) * len(blocks),
        scratch_shapes=[pltpu.VMEM(w.shape, w.dtype) for w in weights]
        + [
            pltpu.VMEM((held, total // held, model + LANES), jnp.bfloat16),
            pltpu.SemaphoreType.DMA((len(weights), held)),
        ],
        compiler_params=pltpu.CompilerParams(vmem_limit_bytes=46 * 1024 * 1024),
        cost_estimate=pl.CostEstimate(
            flops=12 * total * model * hidden,
            bytes_accessed=12 * held * model * hidden,
            transcendentals=2 * total * hidden,
        ),
        name="experts",
    )(first, *blocks, *weights)


def balanced(
    queries,
    key_pairs,
    head_values,
    lambdas,
    head_gain,
    out_weight,
    residual,
    norm_gain,
    expert_ids,
    route_weights,
    gate_weight,
    up_weight,
    down_weight,
):
    tokens, heads, width = queries.shape
    rows, _ = residual.shape
    sp_count, tp_count = lax.axis_size("sp"), lax.axis_size("tp")
    sp_index = lax.axis_index("sp")
    parts = sp_count // heads
    sub = rows // parts
    held = gate_weight.shape[0]
    experts = held * sp_count

    swap = [(i, i ^ 1) for i in range(tp_count)]
    mine = (gate_weight, up_weight, down_weight)
    other = tuple(lax.ppermute(w, "tp", swap) for w in mine)

    split = jnp.transpose(
        queries.reshape(tp_count, parts, sub, heads, width), (1, 3, 0, 2, 4)
    ).reshape(sp_count, tokens // parts, width)
    keys = jnp.tile(jnp.transpose(key_pairs, (1, 0, 2)), (parts, 1, 1))
    values = jnp.tile(jnp.transpose(head_values, (1, 0, 2)), (parts, 1, 1))
    arrived = lax.all_to_all(
        jnp.concatenate([split, keys, values], axis=1), "sp", split_axis=0, concat_axis=0, tiled=True
    )
    attended = attention(
        (sp_index // heads).reshape(1),
        lax.dynamic_slice_in_dim(lambdas, sp_index % heads, 1),
        head_gain.reshape(1, -1),
        arrived,
        sub,
        tokens,
        parts,
        (width // 2) ** (-0.5),
    )
    regrouped = lax.all_to_all(
        attended.reshape(sp_count * tp_count, sub, width),
        ("sp", "tp"),
        split_axis=0,
        concat_axis=0,
        tiled=True,
    ).reshape(sp_count, tp_count, sub, width)

    share = jnp.sum(
        jnp.where(
            expert_ids[:, :, None] == jnp.arange(experts, dtype=jnp.int32),
            route_weights[:, :, None],
            0.0,
        ),
        axis=1,
    )
    coarse = lax.reduce_precision(share, 8, 7)
    named = jnp.any(
        expert_ids[:, :, None] == jnp.arange(experts, dtype=jnp.int32), axis=1
    ).astype(jnp.float32)
    earlier = jnp.tril(jnp.ones((rows, rows), jnp.float32), -1)
    ranks = jnp.where(named > 0, jnp.dot(earlier, named), -1.0)
    routes = jnp.concatenate(
        [coarse, share - coarse, ranks, jnp.zeros((rows, LANES - 3 * experts), jnp.float32)], axis=1
    ).astype(jnp.bfloat16)
    updated, normed = project(
        regrouped, out_weight, residual, norm_gain.reshape(1, -1), routes, parts
    )

    def turn(k):
        return [(i, (i + 2 * k) % tp_count) for i in range(tp_count)]

    def across(array, column):
        return lax.ppermute(array, "sp", [(i, i ^ column) for i in range(sp_count)])

    layers = tp_count // 2
    capacity = row_capacity(rows, expert_ids.shape[1], experts)
    place = sp_index.reshape(1)
    first = (sp_index * held).reshape(1)
    weights = (*mine, *other)
    blocks = [normed] + [lax.ppermute(normed, "tp", turn(-k)) for k in range(1, layers)]
    chosen, arrivals = [], []
    for block in blocks:
        table, *sent = choose(place, block, sp_count, held, experts, capacity)
        chosen.append(table)
        arrivals.append([sent[0]] + [across(sent[c], c) for c in range(1, sp_count)])
    results = {}
    near = near_first(layers)
    for group in ((0, near[0]), near[1:]):
        rows_in = [block for k in group for block in arrivals[k]]
        done = expert_pass(first, rows_in, weights, experts)
        for i, k in enumerate(group):
            results[k] = done[i * sp_count : (i + 1) * sp_count]
    reduced = []
    for k in range(layers):
        result = results[k]
        back = [result[0]] + [across(result[c], c) for c in range(1, sp_count)]
        reduced.append(merge(chosen[k], back))
    returned = [lax.ppermute(reduced[k], "tp", turn(k)) for k in range(1, layers)]
    return summed_rows(updated, reduced[0], *returned)


def row_capacity(rows, routes, experts):
    return max(2, 4 * rows * routes // (3 * experts))


def shards(
    queries,
    key_pairs,
    head_values,
    lambdas,
    head_gain,
    out_weight,
    residual,
    norm_gain,
    expert_ids,
    route_weights,
    gate_weight,
    up_weight,
    down_weight,
):
    tokens_here, heads_here, pair_width = queries.shape
    half_width = pair_width // 2
    value_width = head_values.shape[2]
    score_scale = half_width ** (-0.5)
    query_pos = lax.axis_index("sp") * tokens_here + jnp.arange(tokens_here, dtype=jnp.int32)
    split_queries = queries.reshape(tokens_here, heads_here, 2, half_width)
    start_state = (
        jnp.full((2, heads_here, tokens_here), -1e30, jnp.float32),
        jnp.zeros((2, heads_here, tokens_here), jnp.float32),
        jnp.zeros((2, heads_here, tokens_here, value_width), jnp.float32),
    )
    key_piece = lax.all_gather(key_pairs, "sp", axis=0, tiled=True)
    value_piece = lax.all_gather(head_values, "sp", axis=0, tiled=True)
    span_rows = key_piece.shape[0]
    width_rows = math.gcd(span_rows, 512)

    def block_step(block_index, state):
        running_max, totals, summed = state
        offset = block_index * width_rows
        key_block = lax.dynamic_slice_in_dim(key_piece, offset, width_rows, 0).reshape(
            width_rows, heads_here, 2, half_width
        )
        value_block = lax.dynamic_slice_in_dim(value_piece, offset, width_rows, 0)
        key_pos = offset + jnp.arange(width_rows, dtype=jnp.int32)
        allowed = key_pos[None, :] <= query_pos[:, None]
        scores = (
            jnp.einsum(
                "qhcd,khcd->chqk", split_queries, key_block, preferred_element_type=jnp.float32
            )
            * score_scale
        )
        scores = jnp.where(allowed[None, None], scores, -jnp.inf)
        fresh_max = jnp.maximum(running_max, jnp.max(scores, axis=3))
        decay = jnp.exp(running_max - fresh_max)
        weights = jnp.exp(scores - fresh_max[..., None])
        totals = totals * decay + jnp.sum(weights, axis=3)
        summed = summed * decay[..., None] + jnp.einsum(
            "chqk,khv->chqv",
            weights.astype(jnp.bfloat16),
            value_block,
            preferred_element_type=jnp.float32,
        )
        return (fresh_max, totals, summed)

    def through(state):
        return lax.fori_loop(0, span_rows // width_rows, block_step, state)

    def untouched(state):
        return state

    _, totals, summed = lax.cond(jnp.int32(0) <= query_pos[-1], through, untouched, start_state)
    mixed = (
        summed[0] / totals[0][..., None] - lambdas[:, None, None] * summed[1] / totals[1][..., None]
    )
    normed_heads = (
        mixed * lax.rsqrt(jnp.mean(mixed * mixed, axis=2, keepdims=True) + 1e-06) * head_gain
    )
    attended = (
        jnp.transpose(normed_heads, (1, 0, 2))
        .reshape(tokens_here, heads_here * value_width)
        .astype(jnp.bfloat16)
    )
    rows_here = residual.shape[0]
    regrouped = lax.all_to_all(attended, "tp", split_axis=0, concat_axis=1, tiled=True)
    projected = jnp.dot(regrouped, out_weight, preferred_element_type=jnp.float32)
    updated = (residual.astype(jnp.float32) + projected).astype(jnp.bfloat16)
    widened = updated.astype(jnp.float32)
    normed = (
        widened * lax.rsqrt(jnp.mean(widened * widened, axis=1, keepdims=True) + 1e-06) * norm_gain
    ).astype(jnp.bfloat16)
    route_count = expert_ids.shape[1]
    local_experts = gate_weight.shape[0]
    sp_count = lax.axis_size("sp")
    expert_count = local_experts * sp_count
    capacity = max(2, 4 * rows_here * route_count // (3 * expert_count))
    model_width = normed.shape[1]
    flat_ids = expert_ids.reshape(-1)
    indicator = (flat_ids[:, None] == jnp.arange(expert_count, dtype=jnp.int32)[None, :]).astype(
        jnp.int32
    )
    ranking = jnp.sum(jnp.cumsum(indicator, axis=0) * indicator, axis=1) - 1
    slots = flat_ids * capacity + ranking
    sources = jnp.arange(rows_here * route_count, dtype=jnp.int32) // route_count
    outgoing = (
        jnp.zeros((expert_count * capacity, model_width), jnp.bfloat16)
        .at[slots]
        .set(normed[sources])
    )
    arrived = lax.all_to_all(
        outgoing.reshape(sp_count, local_experts, capacity, model_width),
        "sp",
        split_axis=0,
        concat_axis=0,
        tiled=True,
    )
    piece_rows = lax.all_gather(arrived[None], "tp", axis=0, tiled=True)
    gate_part = jnp.einsum(
        "tsecd,edf->tsecf", piece_rows, gate_weight, preferred_element_type=jnp.float32
    )
    up_part = jnp.einsum(
        "tsecd,edf->tsecf", piece_rows, up_weight, preferred_element_type=jnp.float32
    )
    inner_rows = (jax.nn.silu(gate_part) * up_part).astype(jnp.bfloat16)
    partial_value = jnp.einsum(
        "tsecf,efd->tsecd", inner_rows, down_weight, preferred_element_type=jnp.float32
    )
    reduced = lax.psum_scatter(
        partial_value.astype(jnp.bfloat16), "tp", scatter_dimension=0, tiled=True
    )
    returned = lax.all_to_all(reduced[0], "sp", split_axis=0, concat_axis=0, tiled=True)
    picked = (
        returned.reshape(expert_count * capacity, model_width)[slots]
        .astype(jnp.float32)
        .reshape(rows_here, route_count, model_width)
    )
    moe_sum = jnp.sum(picked * route_weights[:, :, None], axis=1)
    return (updated.astype(jnp.float32) + moe_sum).astype(jnp.bfloat16)


def summed_rows(*terms):
    return sum(term.astype(jnp.float32) for term in terms).astype(jnp.bfloat16)


def near_first(layers):
    return sorted(range(1, layers), key=lambda k: (min(k, layers - k), k))


def fits_balanced(queries, residual, expert_ids, gate_weight, sp_count, tp_count):
    tokens, heads, width = queries.shape
    rows = residual.shape[0]
    held = gate_weight.shape[0]
    if sp_count != 4 or tp_count % 2 or tp_count < 6 or sp_count % heads or width != LANES:
        return False
    sub = rows // (sp_count // heads)
    span = OWNERS_PER_TILE * rows
    capacity = row_capacity(rows, expert_ids.shape[1], held * sp_count)
    return (
        sub % 16 == 0
        and tokens % span == 0
        and span % LANES == 0
        and capacity % 16 == 0
        and 3 * held * sp_count <= LANES
    )


def layer(*args):
    queries, residual, expert_ids, gate_weight = args[0], args[6], args[8], args[10]
    chosen = fits_balanced(
        queries, residual, expert_ids, gate_weight, lax.axis_size("sp"), lax.axis_size("tp")
    )
    return (balanced if chosen else shards)(*args)


def solution(mesh):
    placed = (
        P("sp", "tp", None),
        P("sp", "tp", None),
        P("sp", "tp", None),
        P("tp"),
        P(),
        P(),
        P(("sp", "tp"), None),
        P(),
        P(("sp", "tp"), None),
        P(("sp", "tp"), None),
        P("sp", None, "tp"),
        P("sp", None, "tp"),
        P("sp", "tp", None),
    )
    return jax.shard_map(
        layer, mesh=mesh, in_specs=placed, out_specs=P(("sp", "tp"), None), check_vma=False
    )
```

```python
import functools
import math

import jax
import jax.numpy as jnp
from jax import lax
from jax.experimental import pallas as pl
from jax.experimental.pallas import tpu as pltpu
from jax.sharding import PartitionSpec as P

LANES = 128
KEY_TILE = 256


def attention_kernel(
    part_ref, lam_ref, gain_ref, rows_ref, out_ref, stack_ref, acc_ref, top_ref, *, sub, parts, scale
):
    exact = math.frexp(scale)[0] == 0.5
    tile = pl.program_id(0)
    tile_rows, width = out_ref.shape
    key_rows = tile_rows * parts
    half = width // 2

    query = rows_ref[tile, 0:tile_rows, :]
    if exact:
        query = (query.astype(jnp.float32) * scale).astype(jnp.bfloat16)
    low = lax.broadcasted_iota(jnp.int32, (tile_rows, width), 1) < half
    nothing = jnp.zeros_like(query)
    stack_ref[0:tile_rows, :] = jnp.where(low, query, nothing)
    stack_ref[tile_rows:, :] = jnp.where(low, nothing, query)
    top_ref[...] = jnp.full_like(top_ref, -1e30)
    acc_ref[...] = jnp.zeros_like(acc_ref)

    def absorb(source, first, count, keys, masked_from=None):
        place = pl.ds(first, count)
        scores = lax.dot_general(
            stack_ref[place, :],
            rows_ref[source, pl.ds(tile_rows, keys), :],
            (((1,), (1,)), ((), ())),
            preferred_element_type=jnp.float32,
        )
        if not exact:
            scores = scores * scale
        if masked_from is not None:
            row = lax.broadcasted_iota(jnp.int32, (count, LANES), 0) + masked_from
            where = row + part_ref[0] * sub
            for step in range(1, tile_rows // sub):
                if masked_from < (step + 1) * sub and masked_from + count > step * sub:
                    where = where + jnp.where(row >= step * sub, (parts - 1) * sub, 0)
                elif masked_from >= step * sub:
                    where = where + (parts - 1) * sub
            gap = where - lax.broadcasted_iota(jnp.int32, (count, LANES), 1)
            scores = jnp.concatenate(
                [
                    jnp.where(gap >= start, scores[:, start : start + LANES], -jnp.inf)
                    for start in range(0, keys, LANES)
                ],
                axis=1,
            )
        before = top_ref[place, :]
        after = jnp.maximum(before, jnp.max(scores, axis=1, keepdims=True))
        decay = jnp.exp(before - after)
        weights = jnp.exp(scores - jnp.concatenate([after] * (keys // LANES), axis=1))
        top_ref[place, :] = after
        values = rows_ref[source, pl.ds(tile_rows + key_rows, keys), :]
        acc_ref[place, :] = acc_ref[place, :] * jnp.concatenate(
            [decay] * (1 + width // LANES), axis=1
        ) + jnp.dot(
            weights.astype(jnp.bfloat16),
            jnp.concatenate([values, jnp.ones((keys, LANES), jnp.bfloat16)], axis=1),
            preferred_element_type=jnp.float32,
        )

    chunk = tile_rows // 2

    @pl.loop(0, tile)
    def _(source):
        for first in range(0, 2 * tile_rows, chunk):
            absorb(source, first, chunk, key_rows)

    needed = [
        -(-(owner + 1) * sub * parts // KEY_TILE) * KEY_TILE for owner in range(tile_rows // sub)
    ]
    for keys in sorted(set(needed)):
        owners = [owner for owner in range(len(needed)) if needed[owner] == keys]
        for base in (0, tile_rows):
            absorb(tile, base + owners[0] * sub, len(owners) * sub, keys, owners[0] * sub)

    first = acc_ref[0:tile_rows, :]
    second = acc_ref[tile_rows:, :]
    mixed = first[:, :width] / first[:, width:] - lam_ref[0] * second[:, :width] / second[:, width:]
    scaled = mixed * lax.rsqrt(jnp.mean(mixed * mixed, axis=1, keepdims=True) + 1e-06)
    out_ref[...] = (scaled * gain_ref[...]).astype(out_ref.dtype)


def attention(part, lam, gain, arrived, sub, tile_rows, parts, scale):
    sources, _, width = arrived.shape
    total_rows = sources * tile_rows
    pairs = total_rows * total_rows * parts
    return pl.pallas_call(
        functools.partial(attention_kernel, sub=sub, parts=parts, scale=scale),
        grid=(sources,),
        out_shape=jax.ShapeDtypeStruct((total_rows, width), jnp.bfloat16),
        in_specs=[
            pl.BlockSpec(memory_space=pltpu.SMEM),
            pl.BlockSpec(memory_space=pltpu.SMEM),
            pl.BlockSpec((1, width), lambda i: (0, 0)),
            pl.BlockSpec(memory_space=pltpu.VMEM),
        ],
        out_specs=pl.BlockSpec((tile_rows, width), lambda i: (i, 0)),
        scratch_shapes=[
            pltpu.VMEM((2 * tile_rows, width), jnp.bfloat16),
            pltpu.VMEM((2 * tile_rows, width + LANES), jnp.float32),
            pltpu.VMEM((2 * tile_rows, LANES), jnp.float32),
        ],
        compiler_params=pltpu.CompilerParams(vmem_limit_bytes=20 * 1024 * 1024),
        cost_estimate=pl.CostEstimate(
            flops=8 * pairs * width, bytes_accessed=2 * arrived.size, transcendentals=pairs
        ),
        name="attention",
    )(part, lam, gain, arrived)


def project_kernel(
    heads_ref, weight_ref, residual_ref, gain_ref, routes_ref, updated_ref, normed_ref, left_ref, kept_ref, acc_ref, sems, *, parts
):
    sources, columns, sub, width = heads_ref.shape
    held = sources // parts
    depth = held * width
    copies = [
        pltpu.make_async_copy(
            weight_ref.at[pl.ds(column * depth, depth)], kept_ref.at[column], sems.at[column]
        )
        for column in range(columns)
    ]
    for copy in copies:
        copy.start()
    for part in range(parts):
        for column in range(columns):
            for head in range(held):
                left_ref[
                    column, part * sub : (part + 1) * sub, head * width : (head + 1) * width
                ] = heads_ref[part * held + head, column]
    for column, copy in enumerate(copies):
        copy.wait()
        product = jnp.dot(left_ref[column], kept_ref[column], preferred_element_type=jnp.float32)
        if column == 0:
            acc_ref[...] = residual_ref[...].astype(jnp.float32) + product
        else:
            acc_ref[...] += product
    updated = acc_ref[...].astype(jnp.bfloat16)
    updated_ref[...] = updated
    wide = updated.astype(jnp.float32)
    scaled = wide * lax.rsqrt(jnp.mean(wide * wide, axis=1, keepdims=True) + 1e-06)
    model = wide.shape[1]
    normed_ref[:, :model] = (scaled * gain_ref[...]).astype(jnp.bfloat16)
    normed_ref[:, model:] = routes_ref[...]


def project(heads, out_weight, residual, gain, routes, parts):
    sources, columns, _, width = heads.shape
    rows, model = residual.shape
    depth = sources // parts * width
    whole = pl.BlockSpec(memory_space=pltpu.VMEM)
    return pl.pallas_call(
        functools.partial(project_kernel, parts=parts),
        out_shape=(
            jax.ShapeDtypeStruct((rows, model), jnp.bfloat16),
            jax.ShapeDtypeStruct((rows, model + LANES), jnp.bfloat16),
        ),
        in_specs=[whole, pl.BlockSpec(memory_space=pl.ANY), whole, whole, whole],
        out_specs=(whole, whole),
        scratch_shapes=[
            pltpu.VMEM((columns, rows, depth), jnp.bfloat16),
            pltpu.VMEM((columns, depth, model), jnp.bfloat16),
            pltpu.VMEM((rows, model), jnp.float32),
            pltpu.SemaphoreType.DMA((columns,)),
        ],
        compiler_params=pltpu.CompilerParams(vmem_limit_bytes=56 * 1024 * 1024),
        cost_estimate=pl.CostEstimate(
            flops=2 * rows * out_weight.size, bytes_accessed=2 * out_weight.size, transcendentals=0
        ),
        name="project",
    )(heads, out_weight, residual, gain, routes)


def choose_kernel(place_ref, block_ref, coarse_ref, fine_ref, *out_refs, held, experts, capacity):
    model = block_ref.shape[1] - LANES
    slots = len(out_refs) * held * capacity
    source = lax.broadcasted_iota(jnp.int32, (LANES, slots), 0)
    slot = lax.broadcasted_iota(jnp.int32, (LANES, slots), 1)
    wanted = 0 * slot
    for column in range(len(out_refs)):
        for expert in range(held):
            first = (column * held + expert) * capacity
            name = jnp.bitwise_xor(place_ref[0], column) * held + expert
            inside = (slot >= first) & (slot < first + capacity)
            wanted = jnp.where(inside, name, wanted)

    def looked_up(group):
        table = jnp.where(source == wanted + group * experts, 1.0, 0.0).astype(jnp.bfloat16)
        return jnp.dot(block_ref[:, model:], table, preferred_element_type=jnp.float32)

    ranks = looked_up(2)
    lane = lax.broadcasted_iota(jnp.int32, ranks.shape, 1)
    hit = ranks == lax.rem(lane, capacity).astype(jnp.float32)
    coarse_ref[...] = jnp.where(hit, looked_up(0), 0.0).astype(jnp.bfloat16)
    fine_ref[...] = jnp.where(hit, looked_up(1), 0.0).astype(jnp.bfloat16)
    rows = lax.dot_general(
        jnp.where(hit, 1.0, 0.0).astype(jnp.bfloat16),
        block_ref[:, :model],
        (((0,), (0,)), ((), ())),
        preferred_element_type=jnp.float32,
    ).astype(jnp.bfloat16)
    for column, out_ref in enumerate(out_refs):
        out_ref[...] = rows[column * held * capacity : (column + 1) * held * capacity]


def choose(place, block, columns, held, experts, capacity):
    rows, width = block.shape
    slots = held * capacity
    whole = pl.BlockSpec(memory_space=pltpu.VMEM)
    table = jax.ShapeDtypeStruct((rows, columns * slots), jnp.bfloat16)
    return pl.pallas_call(
        functools.partial(choose_kernel, held=held, experts=experts, capacity=capacity),
        out_shape=(
            table,
            table,
            *(jax.ShapeDtypeStruct((slots, width - LANES), jnp.bfloat16) for _ in range(columns)),
        ),
        in_specs=[pl.BlockSpec(memory_space=pltpu.SMEM), whole],
        out_specs=(whole,) * (columns + 2),
        compiler_params=pltpu.CompilerParams(vmem_limit_bytes=16 * 1024 * 1024),
        cost_estimate=pl.CostEstimate(
            flops=2 * rows * width * columns * slots, bytes_accessed=4 * rows * width, transcendentals=0
        ),
        name="choose",
    )(place, block)


def merge_kernel(coarse_ref, fine_ref, *refs):
    out_ref, kept_ref = refs[-2:]
    slots = refs[0].shape[0]
    for column, ref in enumerate(refs[:-2]):
        kept_ref[column * slots : (column + 1) * slots, :] = ref[...]
    kept = kept_ref[...]
    total = jnp.dot(coarse_ref[...], kept, preferred_element_type=jnp.float32)
    total += jnp.dot(fine_ref[...], kept, preferred_element_type=jnp.float32)
    out_ref[...] = total.astype(out_ref.dtype)


def merge(coarse, fine, parts):
    rows = coarse.shape[0]
    model = parts[0].shape[1]
    whole = pl.BlockSpec(memory_space=pltpu.VMEM)
    return pl.pallas_call(
        merge_kernel,
        out_shape=jax.ShapeDtypeStruct((rows, model), jnp.bfloat16),
        in_specs=[whole] * (2 + len(parts)),
        out_specs=whole,
        scratch_shapes=[pltpu.VMEM((coarse.shape[1], model), jnp.bfloat16)],
        compiler_params=pltpu.CompilerParams(vmem_limit_bytes=16 * 1024 * 1024),
        cost_estimate=pl.CostEstimate(
            flops=4 * rows * coarse.shape[1] * model, bytes_accessed=4 * rows * model, transcendentals=0
        ),
        name="merge",
    )(coarse, fine, *parts)


def expert_kernel(*refs, blocks):
    block_refs = refs[:blocks]
    weight_refs = refs[blocks : 6 + blocks]
    out_refs = refs[6 + blocks : 6 + 2 * blocks]
    kept_refs = refs[6 + 2 * blocks : 12 + 2 * blocks]
    rows_ref, sems = refs[12 + 2 * blocks :]
    held = kept_refs[0].shape[0]
    capacity = block_refs[0].shape[0] // held
    sets = ((0, 1, 2), (3, 4, 5))

    def copy(index, expert):
        return pltpu.make_async_copy(
            weight_refs[index].at[expert], kept_refs[index].at[expert], sems.at[index, expert]
        )

    for expert in range(held):
        for indices in sets:
            for index in indices:
                copy(index, expert).start()

    for expert in range(held):
        for number, ref in enumerate(block_refs):
            rows_ref[expert, number * capacity : (number + 1) * capacity, :] = ref[
                expert * capacity : (expert + 1) * capacity, :
            ]

    for expert in range(held):
        rows = rows_ref[expert]
        total = None
        for indices in sets:
            parts = []
            for index in indices[:2]:
                copy(index, expert).wait()
                parts.append(
                    jnp.dot(rows, kept_refs[index][expert], preferred_element_type=jnp.float32)
                )
            gate, up = parts
            inner = (gate / (1.0 + jnp.exp(-gate)) * up).astype(jnp.bfloat16)
            copy(indices[2], expert).wait()
            term = jnp.dot(inner, kept_refs[indices[2]][expert], preferred_element_type=jnp.float32)
            total = term if total is None else total + term
        total = total.astype(jnp.bfloat16)
        for number, ref in enumerate(out_refs):
            ref[expert * capacity : (expert + 1) * capacity, :] = total[
                number * capacity : (number + 1) * capacity
            ]


def expert_pass(blocks, weights):
    held, model, hidden = weights[0].shape
    slots = blocks[0].shape[0]
    total = len(blocks) * slots
    whole = pl.BlockSpec(memory_space=pltpu.VMEM)
    return pl.pallas_call(
        functools.partial(expert_kernel, blocks=len(blocks)),
        out_shape=tuple(jax.ShapeDtypeStruct((slots, model), jnp.bfloat16) for _ in blocks),
        in_specs=[whole] * len(blocks)
        + [pl.BlockSpec(memory_space=pl.ANY)] * len(weights),
        out_specs=(whole,) * len(blocks),
        scratch_shapes=[pltpu.VMEM(w.shape, w.dtype) for w in weights]
        + [
            pltpu.VMEM((held, total // held, model), jnp.bfloat16),
            pltpu.SemaphoreType.DMA((len(weights), held)),
        ],
        compiler_params=pltpu.CompilerParams(vmem_limit_bytes=46 * 1024 * 1024),
        cost_estimate=pl.CostEstimate(
            flops=12 * total * model * hidden,
            bytes_accessed=12 * held * model * hidden,
            transcendentals=2 * total * hidden,
        ),
        name="experts",
    )(*blocks, *weights)


def balanced(
    queries,
    key_pairs,
    head_values,
    lambdas,
    head_gain,
    out_weight,
    residual,
    norm_gain,
    expert_ids,
    route_weights,
    gate_weight,
    up_weight,
    down_weight,
):
    tokens, heads, width = queries.shape
    rows, _ = residual.shape
    sp_count, tp_count = lax.axis_size("sp"), lax.axis_size("tp")
    sp_index = lax.axis_index("sp")
    parts = sp_count // heads
    sub = rows // parts
    held = gate_weight.shape[0]
    experts = held * sp_count

    swap = [(i, i ^ 1) for i in range(tp_count)]
    mine = (gate_weight, up_weight, down_weight)
    other = tuple(lax.ppermute(w, "tp", swap) for w in mine)

    split = jnp.transpose(
        queries.reshape(tp_count, parts, sub, heads, width), (1, 3, 0, 2, 4)
    ).reshape(sp_count, tokens // parts, width)
    keys = jnp.tile(jnp.transpose(key_pairs, (1, 0, 2)), (parts, 1, 1))
    values = jnp.tile(jnp.transpose(head_values, (1, 0, 2)), (parts, 1, 1))
    arrived = lax.all_to_all(
        jnp.concatenate([split, keys, values], axis=1), "sp", split_axis=0, concat_axis=0, tiled=True
    )
    attended = attention(
        (sp_index // heads).reshape(1),
        lax.dynamic_slice_in_dim(lambdas, sp_index % heads, 1),
        head_gain.reshape(1, -1),
        arrived,
        sub,
        tokens // parts,
        parts,
        (width // 2) ** (-0.5),
    )
    regrouped = lax.all_to_all(
        attended.reshape(sp_count * tp_count, sub, width),
        ("sp", "tp"),
        split_axis=0,
        concat_axis=0,
        tiled=True,
    ).reshape(sp_count, tp_count, sub, width)

    share = jnp.sum(
        jnp.where(
            expert_ids[:, :, None] == jnp.arange(experts, dtype=jnp.int32),
            route_weights[:, :, None],
            0.0,
        ),
        axis=1,
    )
    coarse = lax.reduce_precision(share, 8, 7)
    named = jnp.any(
        expert_ids[:, :, None] == jnp.arange(experts, dtype=jnp.int32), axis=1
    ).astype(jnp.float32)
    earlier = jnp.tril(jnp.ones((rows, rows), jnp.float32), -1)
    ranks = jnp.where(named > 0, jnp.dot(earlier, named), -1.0)
    routes = jnp.concatenate(
        [coarse, share - coarse, ranks, jnp.zeros((rows, LANES - 3 * experts), jnp.float32)], axis=1
    ).astype(jnp.bfloat16)
    updated, normed = project(
        regrouped, out_weight, residual, norm_gain.reshape(1, -1), routes, parts
    )

    def turn(k):
        return [(i, (i + 2 * k) % tp_count) for i in range(tp_count)]

    def across(array, column):
        return lax.ppermute(array, "sp", [(i, i ^ column) for i in range(sp_count)])

    layers = tp_count // 2
    capacity = row_capacity(rows, expert_ids.shape[1], experts)
    place = sp_index.reshape(1)
    weights = (*mine, *other)
    blocks = [normed] + [lax.ppermute(normed, "tp", turn(-k)) for k in range(1, layers)]
    chosen, arrivals = [], []
    for block in blocks:
        coarse, fine, *sent = choose(place, block, sp_count, held, experts, capacity)
        chosen.append((coarse, fine))
        arrivals.append([sent[0]] + [across(sent[c], c) for c in range(1, sp_count)])
    results = {}
    near = near_first(layers)
    for group in ((0, near[0]), near[1:]):
        rows_in = [block for k in group for block in arrivals[k]]
        done = expert_pass(rows_in, weights)
        for i, k in enumerate(group):
            results[k] = done[i * sp_count : (i + 1) * sp_count]
    reduced = []
    for k in range(layers):
        result = results[k]
        back = [result[0]] + [across(result[c], c) for c in range(1, sp_count)]
        reduced.append(merge(*chosen[k], back))
    returned = [lax.ppermute(reduced[k], "tp", turn(k)) for k in range(1, layers)]
    return summed_rows(updated, reduced[0], *returned)


def row_capacity(rows, routes, experts):
    return max(2, 4 * rows * routes // (3 * experts))


def shards(
    queries,
    key_pairs,
    head_values,
    lambdas,
    head_gain,
    out_weight,
    residual,
    norm_gain,
    expert_ids,
    route_weights,
    gate_weight,
    up_weight,
    down_weight,
):
    tokens_here, heads_here, pair_width = queries.shape
    half_width = pair_width // 2
    value_width = head_values.shape[2]
    score_scale = half_width ** (-0.5)
    query_pos = lax.axis_index("sp") * tokens_here + jnp.arange(tokens_here, dtype=jnp.int32)
    split_queries = queries.reshape(tokens_here, heads_here, 2, half_width)
    start_state = (
        jnp.full((2, heads_here, tokens_here), -1e30, jnp.float32),
        jnp.zeros((2, heads_here, tokens_here), jnp.float32),
        jnp.zeros((2, heads_here, tokens_here, value_width), jnp.float32),
    )
    key_piece = lax.all_gather(key_pairs, "sp", axis=0, tiled=True)
    value_piece = lax.all_gather(head_values, "sp", axis=0, tiled=True)
    span_rows = key_piece.shape[0]
    width_rows = math.gcd(span_rows, 512)

    def block_step(block_index, state):
        running_max, totals, summed = state
        offset = block_index * width_rows
        key_block = lax.dynamic_slice_in_dim(key_piece, offset, width_rows, 0).reshape(
            width_rows, heads_here, 2, half_width
        )
        value_block = lax.dynamic_slice_in_dim(value_piece, offset, width_rows, 0)
        key_pos = offset + jnp.arange(width_rows, dtype=jnp.int32)
        allowed = key_pos[None, :] <= query_pos[:, None]
        scores = (
            jnp.einsum(
                "qhcd,khcd->chqk", split_queries, key_block, preferred_element_type=jnp.float32
            )
            * score_scale
        )
        scores = jnp.where(allowed[None, None], scores, -jnp.inf)
        fresh_max = jnp.maximum(running_max, jnp.max(scores, axis=3))
        decay = jnp.exp(running_max - fresh_max)
        weights = jnp.exp(scores - fresh_max[..., None])
        totals = totals * decay + jnp.sum(weights, axis=3)
        summed = summed * decay[..., None] + jnp.einsum(
            "chqk,khv->chqv",
            weights.astype(jnp.bfloat16),
            value_block,
            preferred_element_type=jnp.float32,
        )
        return (fresh_max, totals, summed)

    def through(state):
        return lax.fori_loop(0, span_rows // width_rows, block_step, state)

    def untouched(state):
        return state

    _, totals, summed = lax.cond(jnp.int32(0) <= query_pos[-1], through, untouched, start_state)
    mixed = (
        summed[0] / totals[0][..., None] - lambdas[:, None, None] * summed[1] / totals[1][..., None]
    )
    normed_heads = (
        mixed * lax.rsqrt(jnp.mean(mixed * mixed, axis=2, keepdims=True) + 1e-06) * head_gain
    )
    attended = (
        jnp.transpose(normed_heads, (1, 0, 2))
        .reshape(tokens_here, heads_here * value_width)
        .astype(jnp.bfloat16)
    )
    rows_here = residual.shape[0]
    regrouped = lax.all_to_all(attended, "tp", split_axis=0, concat_axis=1, tiled=True)
    projected = jnp.dot(regrouped, out_weight, preferred_element_type=jnp.float32)
    updated = (residual.astype(jnp.float32) + projected).astype(jnp.bfloat16)
    widened = updated.astype(jnp.float32)
    normed = (
        widened * lax.rsqrt(jnp.mean(widened * widened, axis=1, keepdims=True) + 1e-06) * norm_gain
    ).astype(jnp.bfloat16)
    route_count = expert_ids.shape[1]
    local_experts = gate_weight.shape[0]
    sp_count = lax.axis_size("sp")
    expert_count = local_experts * sp_count
    capacity = max(2, 4 * rows_here * route_count // (3 * expert_count))
    model_width = normed.shape[1]
    flat_ids = expert_ids.reshape(-1)
    indicator = (flat_ids[:, None] == jnp.arange(expert_count, dtype=jnp.int32)[None, :]).astype(
        jnp.int32
    )
    ranking = jnp.sum(jnp.cumsum(indicator, axis=0) * indicator, axis=1) - 1
    slots = flat_ids * capacity + ranking
    sources = jnp.arange(rows_here * route_count, dtype=jnp.int32) // route_count
    outgoing = (
        jnp.zeros((expert_count * capacity, model_width), jnp.bfloat16)
        .at[slots]
        .set(normed[sources])
    )
    arrived = lax.all_to_all(
        outgoing.reshape(sp_count, local_experts, capacity, model_width),
        "sp",
        split_axis=0,
        concat_axis=0,
        tiled=True,
    )
    piece_rows = lax.all_gather(arrived[None], "tp", axis=0, tiled=True)
    gate_part = jnp.einsum(
        "tsecd,edf->tsecf", piece_rows, gate_weight, preferred_element_type=jnp.float32
    )
    up_part = jnp.einsum(
        "tsecd,edf->tsecf", piece_rows, up_weight, preferred_element_type=jnp.float32
    )
    inner_rows = (jax.nn.silu(gate_part) * up_part).astype(jnp.bfloat16)
    partial_value = jnp.einsum(
        "tsecf,efd->tsecd", inner_rows, down_weight, preferred_element_type=jnp.float32
    )
    reduced = lax.psum_scatter(
        partial_value.astype(jnp.bfloat16), "tp", scatter_dimension=0, tiled=True
    )
    returned = lax.all_to_all(reduced[0], "sp", split_axis=0, concat_axis=0, tiled=True)
    picked = (
        returned.reshape(expert_count * capacity, model_width)[slots]
        .astype(jnp.float32)
        .reshape(rows_here, route_count, model_width)
    )
    moe_sum = jnp.sum(picked * route_weights[:, :, None], axis=1)
    return (updated.astype(jnp.float32) + moe_sum).astype(jnp.bfloat16)


def summed_rows(*terms):
    return sum(term.astype(jnp.float32) for term in terms).astype(jnp.bfloat16)


def near_first(layers):
    return sorted(range(1, layers), key=lambda k: (min(k, layers - k), k))


def fits_balanced(queries, residual, expert_ids, gate_weight, sp_count, tp_count):
    tokens, heads, width = queries.shape
    rows = residual.shape[0]
    held = gate_weight.shape[0]
    if sp_count != 4 or tp_count % 2 or tp_count < 6 or sp_count % heads or width != LANES:
        return False
    sub = rows // (sp_count // heads)
    capacity = row_capacity(rows, expert_ids.shape[1], held * sp_count)
    return (
        sub % 16 == 0
        and tokens % KEY_TILE == 0
        and tokens == rows * tp_count
        and capacity % 16 == 0
        and 3 * held * sp_count <= LANES
    )


def layer(*args):
    queries, residual, expert_ids, gate_weight = args[0], args[6], args[8], args[10]
    chosen = fits_balanced(
        queries, residual, expert_ids, gate_weight, lax.axis_size("sp"), lax.axis_size("tp")
    )
    return (balanced if chosen else shards)(*args)


def solution(mesh):
    placed = (
        P("sp", "tp", None),
        P("sp", "tp", None),
        P("sp", "tp", None),
        P("tp"),
        P(),
        P(),
        P(("sp", "tp"), None),
        P(),
        P(("sp", "tp"), None),
        P(("sp", "tp"), None),
        P("sp", None, "tp"),
        P("sp", None, "tp"),
        P("sp", "tp", None),
    )
    return jax.shard_map(
        layer, mesh=mesh, in_specs=placed, out_specs=P(("sp", "tp"), None), check_vma=False
    )
```

```python
import functools
import math

import jax
import jax.numpy as jnp
from jax import lax
from jax.experimental import pallas as pl
from jax.experimental.pallas import tpu as pltpu
from jax.sharding import PartitionSpec as P

LANES = 128
KEY_TILE = 256
PROJECT_LIMIT = 48 * 1024 * 1024


def attention_kernel(
    place_ref, part_ref, lam_ref, gain_ref, *refs, columns, sub, parts, scale
):
    arrived_refs = refs[: 3 * columns]
    out_ref, query_ref, key_ref, value_ref, stack_ref, acc_ref, top_ref, sems = refs[3 * columns :]
    exact = math.frexp(scale)[0] == 0.5
    tile = pl.program_id(0)

    @pl.when(tile == 0)
    def _():
        copies = [
            pltpu.make_async_copy(
                arrived_refs[kind * columns + column],
                ref.at[jnp.bitwise_xor(place_ref[0], column)],
                sems.at[kind, column],
            )
            for column in range(columns)
            for kind, ref in enumerate((query_ref, key_ref, value_ref))
        ]
        for copy in copies:
            copy.start()
        for copy in copies:
            copy.wait()

    tile_rows, width = out_ref.shape
    key_rows = tile_rows * parts
    half = width // 2

    query = query_ref[tile]
    if exact:
        query = (query.astype(jnp.float32) * scale).astype(jnp.bfloat16)
    low = lax.broadcasted_iota(jnp.int32, (tile_rows, width), 1) < half
    nothing = jnp.zeros_like(query)
    stack_ref[0:tile_rows, :] = jnp.where(low, query, nothing)
    stack_ref[tile_rows:, :] = jnp.where(low, nothing, query)
    top_ref[...] = jnp.full_like(top_ref, -1e30)
    acc_ref[...] = jnp.zeros_like(acc_ref)

    def absorb(source, first, count, keys, masked_from=None):
        place = pl.ds(first, count)
        scores = lax.dot_general(
            stack_ref[place, :],
            key_ref[source, pl.ds(0, keys), :],
            (((1,), (1,)), ((), ())),
            preferred_element_type=jnp.float32,
        )
        if not exact:
            scores = scores * scale
        if masked_from is not None:
            row = lax.broadcasted_iota(jnp.int32, (count, LANES), 0) + masked_from
            where = row + part_ref[0] * sub
            for step in range(1, tile_rows // sub):
                if masked_from < (step + 1) * sub and masked_from + count > step * sub:
                    where = where + jnp.where(row >= step * sub, (parts - 1) * sub, 0)
                elif masked_from >= step * sub:
                    where = where + (parts - 1) * sub
            gap = where - lax.broadcasted_iota(jnp.int32, (count, LANES), 1)
            scores = jnp.concatenate(
                [
                    jnp.where(gap >= start, scores[:, start : start + LANES], -jnp.inf)
                    for start in range(0, keys, LANES)
                ],
                axis=1,
            )
        before = top_ref[place, :]
        after = jnp.maximum(before, jnp.max(scores, axis=1, keepdims=True))
        decay = jnp.exp(before - after)
        weights = jnp.exp(scores - jnp.concatenate([after] * (keys // LANES), axis=1))
        top_ref[place, :] = after
        values = value_ref[source, pl.ds(0, keys), :]
        acc_ref[place, :] = acc_ref[place, :] * jnp.concatenate(
            [decay] * (1 + width // LANES), axis=1
        ) + jnp.dot(
            weights.astype(jnp.bfloat16),
            jnp.concatenate([values, jnp.ones((keys, LANES), jnp.bfloat16)], axis=1),
            preferred_element_type=jnp.float32,
        )

    chunk = tile_rows // 2

    @pl.loop(0, tile)
    def _(source):
        for first in range(0, 2 * tile_rows, chunk):
            absorb(source, first, chunk, key_rows)

    needed = [
        -(-(owner + 1) * sub * parts // KEY_TILE) * KEY_TILE for owner in range(tile_rows // sub)
    ]
    for keys in sorted(set(needed)):
        owners = [owner for owner in range(len(needed)) if needed[owner] == keys]
        for base in (0, tile_rows):
            absorb(tile, base + owners[0] * sub, len(owners) * sub, keys, owners[0] * sub)

    first = acc_ref[0:tile_rows, :]
    second = acc_ref[tile_rows:, :]
    mixed = first[:, :width] / first[:, width:] - lam_ref[0] * second[:, :width] / second[:, width:]
    scaled = mixed * lax.rsqrt(jnp.mean(mixed * mixed, axis=1, keepdims=True) + 1e-06)
    out_ref[...] = (scaled * gain_ref[...]).astype(out_ref.dtype)


def attention(place, part, lam, gain, queries, keys, values, sub, parts, scale):
    columns = len(queries)
    tile_rows, width = queries[0].shape
    total_rows = columns * tile_rows
    pairs = total_rows * total_rows * parts
    scalar = pl.BlockSpec(memory_space=pltpu.SMEM)
    return pl.pallas_call(
        functools.partial(attention_kernel, columns=columns, sub=sub, parts=parts, scale=scale),
        grid=(columns,),
        out_shape=jax.ShapeDtypeStruct((total_rows, width), jnp.bfloat16),
        in_specs=[
            scalar,
            scalar,
            scalar,
            pl.BlockSpec((1, width), lambda i: (0, 0)),
            *(pl.BlockSpec(memory_space=pl.ANY) for _ in range(3 * columns)),
        ],
        out_specs=pl.BlockSpec((tile_rows, width), lambda i: (i, 0)),
        scratch_shapes=[
            pltpu.VMEM((columns, tile_rows, width), jnp.bfloat16),
            pltpu.VMEM((columns, tile_rows * parts, width), jnp.bfloat16),
            pltpu.VMEM((columns, tile_rows * parts, width), jnp.bfloat16),
            pltpu.VMEM((2 * tile_rows, width), jnp.bfloat16),
            pltpu.VMEM((2 * tile_rows, width + LANES), jnp.float32),
            pltpu.VMEM((2 * tile_rows, LANES), jnp.float32),
            pltpu.SemaphoreType.DMA((3, columns)),
        ],
        compiler_params=pltpu.CompilerParams(vmem_limit_bytes=56 * 1024 * 1024),
        cost_estimate=pl.CostEstimate(
            flops=8 * pairs * width, bytes_accessed=6 * total_rows * width, transcendentals=pairs
        ),
        name="attention",
    )(place, part, lam, gain, *queries, *keys, *values)


def project_kernel(
    place_ref, heads_ref, weight_ref, residual_ref, gain_ref, routes_ref, updated_ref, normed_ref, *refs, parts, held, experts, capacity
):
    *chosen_refs, left_ref, kept_ref, acc_ref, sems = refs
    sources, columns, sub, width = heads_ref.shape
    together = sources // parts
    depth = together * width
    copies = [
        pltpu.make_async_copy(
            weight_ref.at[pl.ds(column * depth, depth)], kept_ref.at[column], sems.at[column]
        )
        for column in range(columns)
    ]
    for copy in copies:
        copy.start()
    for part in range(parts):
        for column in range(columns):
            for head in range(together):
                left_ref[
                    column, part * sub : (part + 1) * sub, head * width : (head + 1) * width
                ] = heads_ref[part * together + head, column]
    for column, copy in enumerate(copies):
        copy.wait()
        product = jnp.dot(left_ref[column], kept_ref[column], preferred_element_type=jnp.float32)
        if column == 0:
            acc_ref[...] = residual_ref[...].astype(jnp.float32) + product
        else:
            acc_ref[...] += product
    updated = acc_ref[...].astype(jnp.bfloat16)
    updated_ref[...] = updated
    wide = updated.astype(jnp.float32)
    scaled = wide * lax.rsqrt(jnp.mean(wide * wide, axis=1, keepdims=True) + 1e-06)
    model = wide.shape[1]
    normed_ref[:, :model] = (scaled * gain_ref[...]).astype(jnp.bfloat16)
    normed_ref[:, model:] = routes_ref[...]
    choose_kernel(place_ref, normed_ref, *chosen_refs, held=held, experts=experts, capacity=capacity)


def project(place, heads, out_weight, residual, gain, routes, parts, held, experts, capacity):
    sources, columns, _, width = heads.shape
    depth = sources // parts * width
    rows, model = residual.shape
    slots = held * capacity
    whole = pl.BlockSpec(memory_space=pltpu.VMEM)
    table = jax.ShapeDtypeStruct((rows, sources * slots), jnp.bfloat16)
    return pl.pallas_call(
        functools.partial(
            project_kernel, parts=parts, held=held, experts=experts, capacity=capacity
        ),
        out_shape=(
            jax.ShapeDtypeStruct((rows, model), jnp.bfloat16),
            jax.ShapeDtypeStruct((rows, model + LANES), jnp.bfloat16),
            table,
            table,
            *(jax.ShapeDtypeStruct((slots, model), jnp.bfloat16) for _ in range(sources)),
        ),
        in_specs=[
            pl.BlockSpec(memory_space=pltpu.SMEM),
            whole,
            pl.BlockSpec(memory_space=pl.ANY),
            whole,
            whole,
            whole,
        ],
        out_specs=(whole,) * (4 + sources),
        scratch_shapes=[
            pltpu.VMEM((columns, rows, depth), jnp.bfloat16),
            pltpu.VMEM((columns, depth, model), jnp.bfloat16),
            pltpu.VMEM((rows, model), jnp.float32),
            pltpu.SemaphoreType.DMA((columns,)),
        ],
        compiler_params=pltpu.CompilerParams(vmem_limit_bytes=PROJECT_LIMIT),
        cost_estimate=pl.CostEstimate(
            flops=2 * rows * out_weight.size, bytes_accessed=2 * out_weight.size, transcendentals=0
        ),
        name="project",
    )(place, heads, out_weight, residual, gain, routes)


def choose_kernel(place_ref, block_ref, coarse_ref, fine_ref, *out_refs, held, experts, capacity):
    model = block_ref.shape[1] - LANES
    slots = len(out_refs) * held * capacity
    source = lax.broadcasted_iota(jnp.int32, (LANES, slots), 0)
    slot = lax.broadcasted_iota(jnp.int32, (LANES, slots), 1)
    wanted = 0 * slot
    for column in range(len(out_refs)):
        for expert in range(held):
            first = (column * held + expert) * capacity
            name = jnp.bitwise_xor(place_ref[0], column) * held + expert
            inside = (slot >= first) & (slot < first + capacity)
            wanted = jnp.where(inside, name, wanted)

    def looked_up(group):
        table = jnp.where(source == wanted + group * experts, 1.0, 0.0).astype(jnp.bfloat16)
        return jnp.dot(block_ref[:, model:], table, preferred_element_type=jnp.float32)

    ranks = looked_up(2)
    lane = lax.broadcasted_iota(jnp.int32, ranks.shape, 1)
    hit = ranks == lax.rem(lane, capacity).astype(jnp.float32)
    coarse_ref[...] = jnp.where(hit, looked_up(0), 0.0).astype(jnp.bfloat16)
    fine_ref[...] = jnp.where(hit, looked_up(1), 0.0).astype(jnp.bfloat16)
    rows = lax.dot_general(
        jnp.where(hit, 1.0, 0.0).astype(jnp.bfloat16),
        block_ref[:, :model],
        (((0,), (0,)), ((), ())),
        preferred_element_type=jnp.float32,
    ).astype(jnp.bfloat16)
    for column, out_ref in enumerate(out_refs):
        out_ref[...] = rows[column * held * capacity : (column + 1) * held * capacity]


def choose(place, block, columns, held, experts, capacity):
    rows, width = block.shape
    slots = held * capacity
    whole = pl.BlockSpec(memory_space=pltpu.VMEM)
    table = jax.ShapeDtypeStruct((rows, columns * slots), jnp.bfloat16)
    return pl.pallas_call(
        functools.partial(choose_kernel, held=held, experts=experts, capacity=capacity),
        out_shape=(
            table,
            table,
            *(jax.ShapeDtypeStruct((slots, width - LANES), jnp.bfloat16) for _ in range(columns)),
        ),
        in_specs=[pl.BlockSpec(memory_space=pltpu.SMEM), whole],
        out_specs=(whole,) * (columns + 2),
        compiler_params=pltpu.CompilerParams(vmem_limit_bytes=16 * 1024 * 1024),
        cost_estimate=pl.CostEstimate(
            flops=2 * rows * width * columns * slots, bytes_accessed=4 * rows * width, transcendentals=0
        ),
        name="choose",
    )(place, block)


def merge_kernel(coarse_ref, fine_ref, *refs):
    out_ref, kept_ref = refs[-2:]
    slots = refs[0].shape[0]
    for column, ref in enumerate(refs[:-2]):
        kept_ref[column * slots : (column + 1) * slots, :] = ref[...]
    kept = kept_ref[...]
    total = jnp.dot(coarse_ref[...], kept, preferred_element_type=jnp.float32)
    total += jnp.dot(fine_ref[...], kept, preferred_element_type=jnp.float32)
    out_ref[...] = total.astype(out_ref.dtype)


def merge(coarse, fine, parts):
    rows = coarse.shape[0]
    model = parts[0].shape[1]
    whole = pl.BlockSpec(memory_space=pltpu.VMEM)
    return pl.pallas_call(
        merge_kernel,
        out_shape=jax.ShapeDtypeStruct((rows, model), jnp.bfloat16),
        in_specs=[whole] * (2 + len(parts)),
        out_specs=whole,
        scratch_shapes=[pltpu.VMEM((coarse.shape[1], model), jnp.bfloat16)],
        compiler_params=pltpu.CompilerParams(vmem_limit_bytes=16 * 1024 * 1024),
        cost_estimate=pl.CostEstimate(
            flops=4 * rows * coarse.shape[1] * model, bytes_accessed=4 * rows * model, transcendentals=0
        ),
        name="merge",
    )(coarse, fine, *parts)


def expert_kernel(*refs, blocks):
    block_refs = refs[:blocks]
    weight_refs = refs[blocks : 6 + blocks]
    out_refs = refs[6 + blocks : 6 + 2 * blocks]
    kept_refs = refs[6 + 2 * blocks : 12 + 2 * blocks]
    rows_ref, sems = refs[12 + 2 * blocks :]
    held = kept_refs[0].shape[0]
    capacity = block_refs[0].shape[0] // held
    sets = ((0, 1, 2), (3, 4, 5))

    def copy(index, expert):
        return pltpu.make_async_copy(
            weight_refs[index].at[expert], kept_refs[index].at[expert], sems.at[index, expert]
        )

    for expert in range(held):
        for indices in sets:
            for index in indices:
                copy(index, expert).start()

    for expert in range(held):
        for number, ref in enumerate(block_refs):
            rows_ref[expert, number * capacity : (number + 1) * capacity, :] = ref[
                expert * capacity : (expert + 1) * capacity, :
            ]

    for expert in range(held):
        rows = rows_ref[expert]
        total = None
        for indices in sets:
            parts = []
            for index in indices[:2]:
                copy(index, expert).wait()
                parts.append(
                    jnp.dot(rows, kept_refs[index][expert], preferred_element_type=jnp.float32)
                )
            gate, up = parts
            inner = (gate / (1.0 + jnp.exp(-gate)) * up).astype(jnp.bfloat16)
            copy(indices[2], expert).wait()
            term = jnp.dot(inner, kept_refs[indices[2]][expert], preferred_element_type=jnp.float32)
            total = term if total is None else total + term
        total = total.astype(jnp.bfloat16)
        for number, ref in enumerate(out_refs):
            ref[expert * capacity : (expert + 1) * capacity, :] = total[
                number * capacity : (number + 1) * capacity
            ]


def expert_pass(blocks, weights):
    held, model, hidden = weights[0].shape
    slots = blocks[0].shape[0]
    total = len(blocks) * slots
    whole = pl.BlockSpec(memory_space=pltpu.VMEM)
    return pl.pallas_call(
        functools.partial(expert_kernel, blocks=len(blocks)),
        out_shape=tuple(jax.ShapeDtypeStruct((slots, model), jnp.bfloat16) for _ in blocks),
        in_specs=[whole] * len(blocks)
        + [pl.BlockSpec(memory_space=pl.ANY)] * len(weights),
        out_specs=(whole,) * len(blocks),
        scratch_shapes=[pltpu.VMEM(w.shape, w.dtype) for w in weights]
        + [
            pltpu.VMEM((held, total // held, model), jnp.bfloat16),
            pltpu.SemaphoreType.DMA((len(weights), held)),
        ],
        compiler_params=pltpu.CompilerParams(vmem_limit_bytes=46 * 1024 * 1024),
        cost_estimate=pl.CostEstimate(
            flops=12 * total * model * hidden,
            bytes_accessed=12 * held * model * hidden,
            transcendentals=2 * total * hidden,
        ),
        name="experts",
    )(*blocks, *weights)


def balanced(
    queries,
    key_pairs,
    head_values,
    lambdas,
    head_gain,
    out_weight,
    residual,
    norm_gain,
    expert_ids,
    route_weights,
    gate_weight,
    up_weight,
    down_weight,
):
    tokens, heads, width = queries.shape
    rows, _ = residual.shape
    sp_count, tp_count = lax.axis_size("sp"), lax.axis_size("tp")
    sp_index = lax.axis_index("sp")
    parts = sp_count // heads
    sub = rows // parts
    held = gate_weight.shape[0]
    experts = held * sp_count

    capacity = row_capacity(rows, expert_ids.shape[1], experts)
    place = sp_index.reshape(1)

    def across(array, column):
        return lax.ppermute(array, "sp", [(i, i ^ column) for i in range(sp_count)])

    def entries(array, count):
        return [
            lax.dynamic_index_in_dim(array, jnp.bitwise_xor(sp_index, c) % count, 0, keepdims=False)
            for c in range(count)
        ]

    def spread(picked):
        count = len(picked)
        return [picked[0]] + [across(picked[c % count], c) for c in range(1, sp_count)]

    values = entries(jnp.transpose(head_values, (1, 0, 2)), heads)
    key_pairs, queries, *values = lax.optimization_barrier((key_pairs, queries, *values))
    keys = entries(jnp.transpose(key_pairs, (1, 0, 2)), heads)
    split = jnp.transpose(
        queries.reshape(tp_count, parts, sub, heads, width), (1, 3, 0, 2, 4)
    ).reshape(sp_count, tokens // parts, width)
    values, keys = spread(values), spread(keys)
    split = spread(entries(split, sp_count))

    swap = [(i, i ^ 1) for i in range(tp_count)]
    mine = (gate_weight, up_weight, down_weight)
    other = tuple(lax.ppermute(w, "tp", swap) for w in mine)

    attended = attention(
        place,
        (sp_index // heads).reshape(1),
        lax.dynamic_slice_in_dim(lambdas, sp_index % heads, 1),
        head_gain.reshape(1, -1),
        split,
        keys,
        values,
        sub,
        parts,
        (width // 2) ** (-0.5),
    )
    regrouped = lax.all_to_all(
        attended.reshape(sp_count * tp_count, sub, width),
        ("sp", "tp"),
        split_axis=0,
        concat_axis=0,
        tiled=True,
    )
    regrouped = regrouped.reshape(sp_count, tp_count, sub, width)

    share = jnp.sum(
        jnp.where(
            expert_ids[:, :, None] == jnp.arange(experts, dtype=jnp.int32),
            route_weights[:, :, None],
            0.0,
        ),
        axis=1,
    )
    coarse = lax.reduce_precision(share, 8, 7)
    named = jnp.any(
        expert_ids[:, :, None] == jnp.arange(experts, dtype=jnp.int32), axis=1
    ).astype(jnp.float32)
    earlier = jnp.tril(jnp.ones((rows, rows), jnp.float32), -1)
    ranks = jnp.where(named > 0, jnp.dot(earlier, named), -1.0)
    routes = jnp.concatenate(
        [coarse, share - coarse, ranks, jnp.zeros((rows, LANES - 3 * experts), jnp.float32)], axis=1
    ).astype(jnp.bfloat16)
    updated, normed, *picked = project(
        place,
        regrouped,
        out_weight,
        residual,
        norm_gain.reshape(1, -1),
        routes,
        parts,
        held,
        experts,
        capacity,
    )

    def turn(k):
        return [(i, (i + 2 * k) % tp_count) for i in range(tp_count)]

    layers = tp_count // 2
    weights = (*mine, *other)
    blocks = [normed] + [lax.ppermute(normed, "tp", turn(-k)) for k in range(1, layers)]
    chosen, arrivals = [], []
    for k, block in enumerate(blocks):
        coarse, fine, *sent = (
            choose(place, block, sp_count, held, experts, capacity) if k else picked
        )
        chosen.append((coarse, fine))
        arrivals.append([sent[0]] + [across(sent[c], c) for c in range(1, sp_count)])
    results = {}
    near = near_first(layers)
    for group in ((0, near[0]), near[1:]):
        rows_in = [block for k in group for block in arrivals[k]]
        done = expert_pass(rows_in, weights)
        for i, k in enumerate(group):
            results[k] = done[i * sp_count : (i + 1) * sp_count]
    reduced = []
    for k in range(layers):
        result = results[k]
        back = [result[0]] + [across(result[c], c) for c in range(1, sp_count)]
        reduced.append(merge(*chosen[k], back))
    returned = [lax.ppermute(reduced[k], "tp", turn(k)) for k in range(1, layers)]
    return summed_rows(updated, reduced[0], *returned)


def row_capacity(rows, routes, experts):
    return max(2, 4 * rows * routes // (3 * experts))


def shards(
    queries,
    key_pairs,
    head_values,
    lambdas,
    head_gain,
    out_weight,
    residual,
    norm_gain,
    expert_ids,
    route_weights,
    gate_weight,
    up_weight,
    down_weight,
):
    tokens_here, heads_here, pair_width = queries.shape
    half_width = pair_width // 2
    value_width = head_values.shape[2]
    score_scale = half_width ** (-0.5)
    query_pos = lax.axis_index("sp") * tokens_here + jnp.arange(tokens_here, dtype=jnp.int32)
    split_queries = queries.reshape(tokens_here, heads_here, 2, half_width)
    start_state = (
        jnp.full((2, heads_here, tokens_here), -1e30, jnp.float32),
        jnp.zeros((2, heads_here, tokens_here), jnp.float32),
        jnp.zeros((2, heads_here, tokens_here, value_width), jnp.float32),
    )
    key_piece = lax.all_gather(key_pairs, "sp", axis=0, tiled=True)
    value_piece = lax.all_gather(head_values, "sp", axis=0, tiled=True)
    span_rows = key_piece.shape[0]
    width_rows = math.gcd(span_rows, 512)

    def block_step(block_index, state):
        running_max, totals, summed = state
        offset = block_index * width_rows
        key_block = lax.dynamic_slice_in_dim(key_piece, offset, width_rows, 0).reshape(
            width_rows, heads_here, 2, half_width
        )
        value_block = lax.dynamic_slice_in_dim(value_piece, offset, width_rows, 0)
        key_pos = offset + jnp.arange(width_rows, dtype=jnp.int32)
        allowed = key_pos[None, :] <= query_pos[:, None]
        scores = (
            jnp.einsum(
                "qhcd,khcd->chqk", split_queries, key_block, preferred_element_type=jnp.float32
            )
            * score_scale
        )
        scores = jnp.where(allowed[None, None], scores, -jnp.inf)
        fresh_max = jnp.maximum(running_max, jnp.max(scores, axis=3))
        decay = jnp.exp(running_max - fresh_max)
        weights = jnp.exp(scores - fresh_max[..., None])
        totals = totals * decay + jnp.sum(weights, axis=3)
        summed = summed * decay[..., None] + jnp.einsum(
            "chqk,khv->chqv",
            weights.astype(jnp.bfloat16),
            value_block,
            preferred_element_type=jnp.float32,
        )
        return (fresh_max, totals, summed)

    def through(state):
        return lax.fori_loop(0, span_rows // width_rows, block_step, state)

    def untouched(state):
        return state

    _, totals, summed = lax.cond(jnp.int32(0) <= query_pos[-1], through, untouched, start_state)
    mixed = (
        summed[0] / totals[0][..., None] - lambdas[:, None, None] * summed[1] / totals[1][..., None]
    )
    normed_heads = (
        mixed * lax.rsqrt(jnp.mean(mixed * mixed, axis=2, keepdims=True) + 1e-06) * head_gain
    )
    attended = (
        jnp.transpose(normed_heads, (1, 0, 2))
        .reshape(tokens_here, heads_here * value_width)
        .astype(jnp.bfloat16)
    )
    rows_here = residual.shape[0]
    regrouped = lax.all_to_all(attended, "tp", split_axis=0, concat_axis=1, tiled=True)
    projected = jnp.dot(regrouped, out_weight, preferred_element_type=jnp.float32)
    updated = (residual.astype(jnp.float32) + projected).astype(jnp.bfloat16)
    widened = updated.astype(jnp.float32)
    normed = (
        widened * lax.rsqrt(jnp.mean(widened * widened, axis=1, keepdims=True) + 1e-06) * norm_gain
    ).astype(jnp.bfloat16)
    route_count = expert_ids.shape[1]
    local_experts = gate_weight.shape[0]
    sp_count = lax.axis_size("sp")
    expert_count = local_experts * sp_count
    capacity = max(2, 4 * rows_here * route_count // (3 * expert_count))
    model_width = normed.shape[1]
    flat_ids = expert_ids.reshape(-1)
    indicator = (flat_ids[:, None] == jnp.arange(expert_count, dtype=jnp.int32)[None, :]).astype(
        jnp.int32
    )
    ranking = jnp.sum(jnp.cumsum(indicator, axis=0) * indicator, axis=1) - 1
    slots = flat_ids * capacity + ranking
    sources = jnp.arange(rows_here * route_count, dtype=jnp.int32) // route_count
    outgoing = (
        jnp.zeros((expert_count * capacity, model_width), jnp.bfloat16)
        .at[slots]
        .set(normed[sources])
    )
    arrived = lax.all_to_all(
        outgoing.reshape(sp_count, local_experts, capacity, model_width),
        "sp",
        split_axis=0,
        concat_axis=0,
        tiled=True,
    )
    piece_rows = lax.all_gather(arrived[None], "tp", axis=0, tiled=True)
    gate_part = jnp.einsum(
        "tsecd,edf->tsecf", piece_rows, gate_weight, preferred_element_type=jnp.float32
    )
    up_part = jnp.einsum(
        "tsecd,edf->tsecf", piece_rows, up_weight, preferred_element_type=jnp.float32
    )
    inner_rows = (jax.nn.silu(gate_part) * up_part).astype(jnp.bfloat16)
    partial_value = jnp.einsum(
        "tsecf,efd->tsecd", inner_rows, down_weight, preferred_element_type=jnp.float32
    )
    reduced = lax.psum_scatter(
        partial_value.astype(jnp.bfloat16), "tp", scatter_dimension=0, tiled=True
    )
    returned = lax.all_to_all(reduced[0], "sp", split_axis=0, concat_axis=0, tiled=True)
    picked = (
        returned.reshape(expert_count * capacity, model_width)[slots]
        .astype(jnp.float32)
        .reshape(rows_here, route_count, model_width)
    )
    moe_sum = jnp.sum(picked * route_weights[:, :, None], axis=1)
    return (updated.astype(jnp.float32) + moe_sum).astype(jnp.bfloat16)


def summed_rows(*terms):
    return sum(term.astype(jnp.float32) for term in terms).astype(jnp.bfloat16)


def near_first(layers):
    return sorted(range(1, layers), key=lambda k: (min(k, layers - k), k))


def fits_balanced(queries, residual, expert_ids, gate_weight, sp_count, tp_count):
    tokens, heads, width = queries.shape
    rows = residual.shape[0]
    held = gate_weight.shape[0]
    if sp_count != 4 or tp_count % 2 or tp_count < 6 or sp_count % heads or width != LANES:
        return False
    sub = rows // (sp_count // heads)
    capacity = row_capacity(rows, expert_ids.shape[1], held * sp_count)
    return (
        sub % 16 == 0
        and tokens % KEY_TILE == 0
        and tokens == rows * tp_count
        and capacity % 16 == 0
        and 3 * held * sp_count <= LANES
    )


def layer(*args):
    queries, residual, expert_ids, gate_weight = args[0], args[6], args[8], args[10]
    chosen = fits_balanced(
        queries, residual, expert_ids, gate_weight, lax.axis_size("sp"), lax.axis_size("tp")
    )
    return (balanced if chosen else shards)(*args)


def solution(mesh):
    placed = (
        P("sp", "tp", None),
        P("sp", "tp", None),
        P("sp", "tp", None),
        P("tp"),
        P(),
        P(),
        P(("sp", "tp"), None),
        P(),
        P(("sp", "tp"), None),
        P(("sp", "tp"), None),
        P("sp", None, "tp"),
        P("sp", None, "tp"),
        P("sp", "tp", None),
    )
    return jax.shard_map(
        layer, mesh=mesh, in_specs=placed, out_specs=P(("sp", "tp"), None), check_vma=False
    )
```

```python
import functools
import math

import jax
import jax.numpy as jnp
from jax import lax
from jax.experimental import pallas as pl
from jax.experimental.pallas import tpu as pltpu
from jax.sharding import PartitionSpec as P

LANES = 128
KEY_TILE = 256
PROJECT_LIMIT = 48 * 1024 * 1024


def attention_kernel(
    place_ref, part_ref, lam_ref, gain_ref, *refs, columns, sub, parts, scale
):
    arrived_refs = refs[: 3 * columns]
    out_ref, query_ref, key_ref, value_ref, stack_ref, acc_ref, top_ref, sems = refs[3 * columns :]
    exact = math.frexp(scale)[0] == 0.5
    tile = pl.program_id(0)

    @pl.when(tile == 0)
    def _():
        copies = [
            pltpu.make_async_copy(
                arrived_refs[kind * columns + column],
                ref.at[jnp.bitwise_xor(place_ref[0], column)],
                sems.at[kind, column],
            )
            for column in range(columns)
            for kind, ref in enumerate((query_ref, key_ref, value_ref))
        ]
        for copy in copies:
            copy.start()
        for copy in copies:
            copy.wait()

    tile_rows, width = out_ref.shape
    key_rows = tile_rows * parts
    half = width // 2

    query = query_ref[tile]
    if exact:
        query = (query.astype(jnp.float32) * scale).astype(jnp.bfloat16)
    low = lax.broadcasted_iota(jnp.int32, (tile_rows, width), 1) < half
    nothing = jnp.zeros_like(query)
    stack_ref[0:tile_rows, :] = jnp.where(low, query, nothing)
    stack_ref[tile_rows:, :] = jnp.where(low, nothing, query)
    top_ref[...] = jnp.full_like(top_ref, -1e30)
    acc_ref[...] = jnp.zeros_like(acc_ref)

    def absorb(source, first, count, keys, masked_from=None):
        place = pl.ds(first, count)
        scores = lax.dot_general(
            stack_ref[place, :],
            key_ref[source, pl.ds(0, keys), :],
            (((1,), (1,)), ((), ())),
            preferred_element_type=jnp.float32,
        )
        if not exact:
            scores = scores * scale
        if masked_from is not None:
            row = lax.broadcasted_iota(jnp.int32, (count, LANES), 0) + masked_from
            where = row + part_ref[0] * sub
            for step in range(1, tile_rows // sub):
                if masked_from < (step + 1) * sub and masked_from + count > step * sub:
                    where = where + jnp.where(row >= step * sub, (parts - 1) * sub, 0)
                elif masked_from >= step * sub:
                    where = where + (parts - 1) * sub
            gap = where - lax.broadcasted_iota(jnp.int32, (count, LANES), 1)
            scores = jnp.concatenate(
                [
                    jnp.where(gap >= start, scores[:, start : start + LANES], -jnp.inf)
                    for start in range(0, keys, LANES)
                ],
                axis=1,
            )
        before = top_ref[place, :]
        after = jnp.maximum(before, jnp.max(scores, axis=1, keepdims=True))
        decay = jnp.exp(before - after)
        weights = jnp.exp(scores - jnp.concatenate([after] * (keys // LANES), axis=1))
        top_ref[place, :] = after
        values = value_ref[source, pl.ds(0, keys), :]
        acc_ref[place, :] = acc_ref[place, :] * jnp.concatenate(
            [decay] * (1 + width // LANES), axis=1
        ) + jnp.dot(
            weights.astype(jnp.bfloat16),
            jnp.concatenate([values, jnp.ones((keys, LANES), jnp.bfloat16)], axis=1),
            preferred_element_type=jnp.float32,
        )

    chunk = tile_rows // 2

    @pl.loop(0, tile)
    def _(source):
        for first in range(0, 2 * tile_rows, chunk):
            absorb(source, first, chunk, key_rows)

    needed = [
        -(-(owner + 1) * sub * parts // KEY_TILE) * KEY_TILE for owner in range(tile_rows // sub)
    ]
    for keys in sorted(set(needed)):
        owners = [owner for owner in range(len(needed)) if needed[owner] == keys]
        for base in (0, tile_rows):
            absorb(tile, base + owners[0] * sub, len(owners) * sub, keys, owners[0] * sub)

    first = acc_ref[0:tile_rows, :]
    second = acc_ref[tile_rows:, :]
    mixed = first[:, :width] / first[:, width:] - lam_ref[0] * second[:, :width] / second[:, width:]
    scaled = mixed * lax.rsqrt(jnp.mean(mixed * mixed, axis=1, keepdims=True) + 1e-06)
    out_ref[...] = (scaled * gain_ref[...]).astype(out_ref.dtype)


def attention(place, part, lam, gain, queries, keys, values, sub, parts, scale):
    columns = len(queries)
    tile_rows, width = queries[0].shape
    total_rows = columns * tile_rows
    pairs = total_rows * total_rows * parts
    scalar = pl.BlockSpec(memory_space=pltpu.SMEM)
    return pl.pallas_call(
        functools.partial(attention_kernel, columns=columns, sub=sub, parts=parts, scale=scale),
        grid=(columns,),
        out_shape=jax.ShapeDtypeStruct((total_rows, width), jnp.bfloat16),
        in_specs=[
            scalar,
            scalar,
            scalar,
            pl.BlockSpec((1, width), lambda i: (0, 0)),
            *(pl.BlockSpec(memory_space=pl.ANY) for _ in range(3 * columns)),
        ],
        out_specs=pl.BlockSpec((tile_rows, width), lambda i: (i, 0)),
        scratch_shapes=[
            pltpu.VMEM((columns, tile_rows, width), jnp.bfloat16),
            pltpu.VMEM((columns, tile_rows * parts, width), jnp.bfloat16),
            pltpu.VMEM((columns, tile_rows * parts, width), jnp.bfloat16),
            pltpu.VMEM((2 * tile_rows, width), jnp.bfloat16),
            pltpu.VMEM((2 * tile_rows, width + LANES), jnp.float32),
            pltpu.VMEM((2 * tile_rows, LANES), jnp.float32),
            pltpu.SemaphoreType.DMA((3, columns)),
        ],
        compiler_params=pltpu.CompilerParams(vmem_limit_bytes=56 * 1024 * 1024),
        cost_estimate=pl.CostEstimate(
            flops=8 * pairs * width, bytes_accessed=6 * total_rows * width, transcendentals=pairs
        ),
        name="attention",
    )(place, part, lam, gain, *queries, *keys, *values)


def project_kernel(
    place_ref, heads_ref, weight_ref, residual_ref, gain_ref, routes_ref, updated_ref, normed_ref, *refs, parts, held, experts, capacity
):
    *chosen_refs, left_ref, kept_ref, acc_ref, sems = refs
    sources, columns, sub, width = heads_ref.shape
    together = sources // parts
    depth = together * width
    copies = [
        pltpu.make_async_copy(
            weight_ref.at[pl.ds(column * depth, depth)], kept_ref.at[column], sems.at[column]
        )
        for column in range(columns)
    ]
    for copy in copies:
        copy.start()
    for part in range(parts):
        for column in range(columns):
            for head in range(together):
                left_ref[
                    column, part * sub : (part + 1) * sub, head * width : (head + 1) * width
                ] = heads_ref[part * together + head, column]
    for column, copy in enumerate(copies):
        copy.wait()
        product = jnp.dot(left_ref[column], kept_ref[column], preferred_element_type=jnp.float32)
        if column == 0:
            acc_ref[...] = residual_ref[...].astype(jnp.float32) + product
        else:
            acc_ref[...] += product
    updated = acc_ref[...].astype(jnp.bfloat16)
    updated_ref[...] = updated
    wide = updated.astype(jnp.float32)
    scaled = wide * lax.rsqrt(jnp.mean(wide * wide, axis=1, keepdims=True) + 1e-06)
    model = wide.shape[1]
    normed_ref[:, :model] = (scaled * gain_ref[...]).astype(jnp.bfloat16)
    normed_ref[:, model:] = routes_ref[...]
    choose_kernel(place_ref, normed_ref, *chosen_refs, held=held, experts=experts, capacity=capacity)


def project(place, heads, out_weight, residual, gain, routes, parts, held, experts, capacity):
    sources, columns, _, width = heads.shape
    depth = sources // parts * width
    rows, model = residual.shape
    slots = held * capacity
    whole = pl.BlockSpec(memory_space=pltpu.VMEM)
    table = jax.ShapeDtypeStruct((rows, sources * slots), jnp.bfloat16)
    return pl.pallas_call(
        functools.partial(
            project_kernel, parts=parts, held=held, experts=experts, capacity=capacity
        ),
        out_shape=(
            jax.ShapeDtypeStruct((rows, model), jnp.bfloat16),
            jax.ShapeDtypeStruct((rows, model + LANES), jnp.bfloat16),
            table,
            table,
            *(jax.ShapeDtypeStruct((slots, model), jnp.bfloat16) for _ in range(sources)),
        ),
        in_specs=[
            pl.BlockSpec(memory_space=pltpu.SMEM),
            whole,
            pl.BlockSpec(memory_space=pl.ANY),
            whole,
            whole,
            whole,
        ],
        out_specs=(whole,) * (4 + sources),
        scratch_shapes=[
            pltpu.VMEM((columns, rows, depth), jnp.bfloat16),
            pltpu.VMEM((columns, depth, model), jnp.bfloat16),
            pltpu.VMEM((rows, model), jnp.float32),
            pltpu.SemaphoreType.DMA((columns,)),
        ],
        compiler_params=pltpu.CompilerParams(vmem_limit_bytes=PROJECT_LIMIT),
        cost_estimate=pl.CostEstimate(
            flops=2 * rows * out_weight.size, bytes_accessed=2 * out_weight.size, transcendentals=0
        ),
        name="project",
    )(place, heads, out_weight, residual, gain, routes)


def choose_kernel(place_ref, block_ref, coarse_ref, fine_ref, *out_refs, held, experts, capacity):
    model = block_ref.shape[1] - LANES
    slots = len(out_refs) * held * capacity
    source = lax.broadcasted_iota(jnp.int32, (LANES, slots), 0)
    slot = lax.broadcasted_iota(jnp.int32, (LANES, slots), 1)
    wanted = 0 * slot
    for column in range(len(out_refs)):
        for expert in range(held):
            first = (column * held + expert) * capacity
            name = jnp.bitwise_xor(place_ref[0], column) * held + expert
            inside = (slot >= first) & (slot < first + capacity)
            wanted = jnp.where(inside, name, wanted)

    def looked_up(group):
        table = jnp.where(source == wanted + group * experts, 1.0, 0.0).astype(jnp.bfloat16)
        return jnp.dot(block_ref[:, model:], table, preferred_element_type=jnp.float32)

    ranks = looked_up(2)
    lane = lax.broadcasted_iota(jnp.int32, ranks.shape, 1)
    hit = ranks == lax.rem(lane, capacity).astype(jnp.float32)
    coarse_ref[...] = jnp.where(hit, looked_up(0), 0.0).astype(jnp.bfloat16)
    fine_ref[...] = jnp.where(hit, looked_up(1), 0.0).astype(jnp.bfloat16)
    rows = lax.dot_general(
        jnp.where(hit, 1.0, 0.0).astype(jnp.bfloat16),
        block_ref[:, :model],
        (((0,), (0,)), ((), ())),
        preferred_element_type=jnp.float32,
    ).astype(jnp.bfloat16)
    for column, out_ref in enumerate(out_refs):
        out_ref[...] = rows[column * held * capacity : (column + 1) * held * capacity]


def choose(place, block, columns, held, experts, capacity):
    rows, width = block.shape
    slots = held * capacity
    whole = pl.BlockSpec(memory_space=pltpu.VMEM)
    table = jax.ShapeDtypeStruct((rows, columns * slots), jnp.bfloat16)
    return pl.pallas_call(
        functools.partial(choose_kernel, held=held, experts=experts, capacity=capacity),
        out_shape=(
            table,
            table,
            *(jax.ShapeDtypeStruct((slots, width - LANES), jnp.bfloat16) for _ in range(columns)),
        ),
        in_specs=[pl.BlockSpec(memory_space=pltpu.SMEM), whole],
        out_specs=(whole,) * (columns + 2),
        compiler_params=pltpu.CompilerParams(vmem_limit_bytes=16 * 1024 * 1024),
        cost_estimate=pl.CostEstimate(
            flops=2 * rows * width * columns * slots, bytes_accessed=4 * rows * width, transcendentals=0
        ),
        name="choose",
    )(place, block)


def merge_kernel(coarse_ref, fine_ref, *refs):
    out_ref, kept_ref = refs[-2:]
    slots = refs[0].shape[0]
    for column, ref in enumerate(refs[:-2]):
        kept_ref[column * slots : (column + 1) * slots, :] = ref[...]
    kept = kept_ref[...]
    used = kept.shape[0]
    total = jnp.dot(coarse_ref[...][:, :used], kept, preferred_element_type=jnp.float32)
    total += jnp.dot(fine_ref[...][:, :used], kept, preferred_element_type=jnp.float32)
    out_ref[...] = total.astype(out_ref.dtype)


def merge(coarse, fine, parts):
    rows = coarse.shape[0]
    model = parts[0].shape[1]
    whole = pl.BlockSpec(memory_space=pltpu.VMEM)
    return pl.pallas_call(
        merge_kernel,
        out_shape=jax.ShapeDtypeStruct((rows, model), jnp.bfloat16),
        in_specs=[whole] * (2 + len(parts)),
        out_specs=whole,
        scratch_shapes=[pltpu.VMEM((len(parts) * parts[0].shape[0], model), jnp.bfloat16)],
        compiler_params=pltpu.CompilerParams(vmem_limit_bytes=16 * 1024 * 1024),
        cost_estimate=pl.CostEstimate(
            flops=4 * rows * coarse.shape[1] * model, bytes_accessed=4 * rows * model, transcendentals=0
        ),
        name="merge",
    )(coarse, fine, *parts)


def expert_kernel(*refs, blocks):
    block_refs = refs[:blocks]
    weight_refs = refs[blocks : 6 + blocks]
    out_refs = refs[6 + blocks : 6 + 2 * blocks]
    kept_refs = refs[6 + 2 * blocks : 12 + 2 * blocks]
    rows_ref, sems = refs[12 + 2 * blocks :]
    held = kept_refs[0].shape[0]
    capacity = block_refs[0].shape[0] // held
    sets = ((0, 1, 2), (3, 4, 5))

    def copy(index, expert):
        return pltpu.make_async_copy(
            weight_refs[index].at[expert], kept_refs[index].at[expert], sems.at[index, expert]
        )

    for expert in range(held):
        for indices in sets:
            for index in indices:
                copy(index, expert).start()

    for expert in range(held):
        for number, ref in enumerate(block_refs):
            rows_ref[expert, number * capacity : (number + 1) * capacity, :] = ref[
                expert * capacity : (expert + 1) * capacity, :
            ]

    for expert in range(held):
        rows = rows_ref[expert]
        total = None
        for indices in sets:
            parts = []
            for index in indices[:2]:
                copy(index, expert).wait()
                parts.append(
                    jnp.dot(rows, kept_refs[index][expert], preferred_element_type=jnp.float32)
                )
            gate, up = parts
            inner = (gate / (1.0 + jnp.exp(-gate)) * up).astype(jnp.bfloat16)
            copy(indices[2], expert).wait()
            term = jnp.dot(inner, kept_refs[indices[2]][expert], preferred_element_type=jnp.float32)
            total = term if total is None else total + term
        total = total.astype(jnp.bfloat16)
        for number, ref in enumerate(out_refs):
            ref[expert * capacity : (expert + 1) * capacity, :] = total[
                number * capacity : (number + 1) * capacity
            ]


def expert_pass(blocks, weights):
    held, model, hidden = weights[0].shape
    slots = blocks[0].shape[0]
    total = len(blocks) * slots
    whole = pl.BlockSpec(memory_space=pltpu.VMEM)
    return pl.pallas_call(
        functools.partial(expert_kernel, blocks=len(blocks)),
        out_shape=tuple(jax.ShapeDtypeStruct((slots, model), jnp.bfloat16) for _ in blocks),
        in_specs=[whole] * len(blocks)
        + [pl.BlockSpec(memory_space=pl.ANY)] * len(weights),
        out_specs=(whole,) * len(blocks),
        scratch_shapes=[pltpu.VMEM(w.shape, w.dtype) for w in weights]
        + [
            pltpu.VMEM((held, total // held, model), jnp.bfloat16),
            pltpu.SemaphoreType.DMA((len(weights), held)),
        ],
        compiler_params=pltpu.CompilerParams(vmem_limit_bytes=46 * 1024 * 1024),
        cost_estimate=pl.CostEstimate(
            flops=12 * total * model * hidden,
            bytes_accessed=12 * held * model * hidden,
            transcendentals=2 * total * hidden,
        ),
        name="experts",
    )(*blocks, *weights)


def balanced(
    queries,
    key_pairs,
    head_values,
    lambdas,
    head_gain,
    out_weight,
    residual,
    norm_gain,
    expert_ids,
    route_weights,
    gate_weight,
    up_weight,
    down_weight,
):
    tokens, heads, width = queries.shape
    rows, _ = residual.shape
    sp_count, tp_count = lax.axis_size("sp"), lax.axis_size("tp")
    sp_index = lax.axis_index("sp")
    parts = sp_count // heads
    sub = rows // parts
    held = gate_weight.shape[0]
    experts = held * sp_count

    capacity = row_capacity(rows, expert_ids.shape[1], experts)
    place = sp_index.reshape(1)

    def across(array, column):
        return lax.ppermute(array, "sp", [(i, i ^ column) for i in range(sp_count)])

    def entries(array, count):
        return [
            lax.dynamic_index_in_dim(array, jnp.bitwise_xor(sp_index, c) % count, 0, keepdims=False)
            for c in range(count)
        ]

    def spread(picked):
        count = len(picked)
        return [picked[0]] + [across(picked[c % count], c) for c in range(1, sp_count)]

    values = entries(jnp.transpose(head_values, (1, 0, 2)), heads)
    key_pairs, queries, *values = lax.optimization_barrier((key_pairs, queries, *values))
    keys = entries(jnp.transpose(key_pairs, (1, 0, 2)), heads)
    split = jnp.transpose(
        queries.reshape(tp_count, parts, sub, heads, width), (1, 3, 0, 2, 4)
    ).reshape(sp_count, tokens // parts, width)
    values, keys = spread(values), spread(keys)
    split = spread(entries(split, sp_count))

    swap = [(i, i ^ 1) for i in range(tp_count)]
    mine = (gate_weight, up_weight, down_weight)
    other = tuple(lax.ppermute(w, "tp", swap) for w in mine)

    attended = attention(
        place,
        (sp_index // heads).reshape(1),
        lax.dynamic_slice_in_dim(lambdas, sp_index % heads, 1),
        head_gain.reshape(1, -1),
        split,
        keys,
        values,
        sub,
        parts,
        (width // 2) ** (-0.5),
    )
    regrouped = lax.all_to_all(
        attended.reshape(sp_count * tp_count, sub, width),
        ("sp", "tp"),
        split_axis=0,
        concat_axis=0,
        tiled=True,
    )
    regrouped = regrouped.reshape(sp_count, tp_count, sub, width)

    share = jnp.sum(
        jnp.where(
            expert_ids[:, :, None] == jnp.arange(experts, dtype=jnp.int32),
            route_weights[:, :, None],
            0.0,
        ),
        axis=1,
    )
    coarse = lax.reduce_precision(share, 8, 7)
    named = jnp.any(
        expert_ids[:, :, None] == jnp.arange(experts, dtype=jnp.int32), axis=1
    ).astype(jnp.float32)
    earlier = jnp.tril(jnp.ones((rows, rows), jnp.float32), -1)
    ranks = jnp.where(named > 0, jnp.dot(earlier, named), -1.0)
    routes = jnp.concatenate(
        [coarse, share - coarse, ranks, jnp.zeros((rows, LANES - 3 * experts), jnp.float32)], axis=1
    ).astype(jnp.bfloat16)
    updated, normed, *picked = project(
        place,
        regrouped,
        out_weight,
        residual,
        norm_gain.reshape(1, -1),
        routes,
        parts,
        held,
        experts,
        capacity,
    )

    def turn(k):
        return [(i, (i + 2 * k) % tp_count) for i in range(tp_count)]

    layers = tp_count // 2
    weights = (*mine, *other)
    blocks = [normed] + [lax.ppermute(normed, "tp", turn(-k)) for k in range(1, layers)]
    chosen, arrivals = [], []
    for k, block in enumerate(blocks):
        coarse, fine, *sent = (
            choose(place, block, sp_count, held, experts, capacity) if k else picked
        )
        chosen.append((coarse, fine))
        arrivals.append([sent[0]] + [across(sent[c], c) for c in range(1, sp_count)])
    results = {}
    near = near_first(layers)
    for group in ((0, near[0]), near[1:]):
        rows_in = [block for k in group for block in arrivals[k]]
        done = expert_pass(rows_in, weights)
        for i, k in enumerate(group):
            results[k] = done[i * sp_count : (i + 1) * sp_count]
    results = {k: list(result) for k, result in results.items()}
    passed = lax.ppermute(results[near[0]].pop(), "tp", turn(near[0]))
    results[0][-1] = summed_rows(results[0][-1], passed)
    reduced = []
    for k in range(layers):
        result = results[k]
        back = [result[0]] + [across(result[c], c) for c in range(1, len(result))]
        reduced.append(merge(*chosen[k], back))
    returned = [lax.ppermute(reduced[k], "tp", turn(k)) for k in range(1, layers)]
    return summed_rows(updated, reduced[0], *returned)


def row_capacity(rows, routes, experts):
    return max(2, 4 * rows * routes // (3 * experts))


def shards(
    queries,
    key_pairs,
    head_values,
    lambdas,
    head_gain,
    out_weight,
    residual,
    norm_gain,
    expert_ids,
    route_weights,
    gate_weight,
    up_weight,
    down_weight,
):
    tokens_here, heads_here, pair_width = queries.shape
    half_width = pair_width // 2
    value_width = head_values.shape[2]
    score_scale = half_width ** (-0.5)
    query_pos = lax.axis_index("sp") * tokens_here + jnp.arange(tokens_here, dtype=jnp.int32)
    split_queries = queries.reshape(tokens_here, heads_here, 2, half_width)
    start_state = (
        jnp.full((2, heads_here, tokens_here), -1e30, jnp.float32),
        jnp.zeros((2, heads_here, tokens_here), jnp.float32),
        jnp.zeros((2, heads_here, tokens_here, value_width), jnp.float32),
    )
    key_piece = lax.all_gather(key_pairs, "sp", axis=0, tiled=True)
    value_piece = lax.all_gather(head_values, "sp", axis=0, tiled=True)
    span_rows = key_piece.shape[0]
    width_rows = math.gcd(span_rows, 512)

    def block_step(block_index, state):
        running_max, totals, summed = state
        offset = block_index * width_rows
        key_block = lax.dynamic_slice_in_dim(key_piece, offset, width_rows, 0).reshape(
            width_rows, heads_here, 2, half_width
        )
        value_block = lax.dynamic_slice_in_dim(value_piece, offset, width_rows, 0)
        key_pos = offset + jnp.arange(width_rows, dtype=jnp.int32)
        allowed = key_pos[None, :] <= query_pos[:, None]
        scores = (
            jnp.einsum(
                "qhcd,khcd->chqk", split_queries, key_block, preferred_element_type=jnp.float32
            )
            * score_scale
        )
        scores = jnp.where(allowed[None, None], scores, -jnp.inf)
        fresh_max = jnp.maximum(running_max, jnp.max(scores, axis=3))
        decay = jnp.exp(running_max - fresh_max)
        weights = jnp.exp(scores - fresh_max[..., None])
        totals = totals * decay + jnp.sum(weights, axis=3)
        summed = summed * decay[..., None] + jnp.einsum(
            "chqk,khv->chqv",
            weights.astype(jnp.bfloat16),
            value_block,
            preferred_element_type=jnp.float32,
        )
        return (fresh_max, totals, summed)

    def through(state):
        return lax.fori_loop(0, span_rows // width_rows, block_step, state)

    def untouched(state):
        return state

    _, totals, summed = lax.cond(jnp.int32(0) <= query_pos[-1], through, untouched, start_state)
    mixed = (
        summed[0] / totals[0][..., None] - lambdas[:, None, None] * summed[1] / totals[1][..., None]
    )
    normed_heads = (
        mixed * lax.rsqrt(jnp.mean(mixed * mixed, axis=2, keepdims=True) + 1e-06) * head_gain
    )
    attended = (
        jnp.transpose(normed_heads, (1, 0, 2))
        .reshape(tokens_here, heads_here * value_width)
        .astype(jnp.bfloat16)
    )
    rows_here = residual.shape[0]
    regrouped = lax.all_to_all(attended, "tp", split_axis=0, concat_axis=1, tiled=True)
    projected = jnp.dot(regrouped, out_weight, preferred_element_type=jnp.float32)
    updated = (residual.astype(jnp.float32) + projected).astype(jnp.bfloat16)
    widened = updated.astype(jnp.float32)
    normed = (
        widened * lax.rsqrt(jnp.mean(widened * widened, axis=1, keepdims=True) + 1e-06) * norm_gain
    ).astype(jnp.bfloat16)
    route_count = expert_ids.shape[1]
    local_experts = gate_weight.shape[0]
    sp_count = lax.axis_size("sp")
    expert_count = local_experts * sp_count
    capacity = max(2, 4 * rows_here * route_count // (3 * expert_count))
    model_width = normed.shape[1]
    flat_ids = expert_ids.reshape(-1)
    indicator = (flat_ids[:, None] == jnp.arange(expert_count, dtype=jnp.int32)[None, :]).astype(
        jnp.int32
    )
    ranking = jnp.sum(jnp.cumsum(indicator, axis=0) * indicator, axis=1) - 1
    slots = flat_ids * capacity + ranking
    sources = jnp.arange(rows_here * route_count, dtype=jnp.int32) // route_count
    outgoing = (
        jnp.zeros((expert_count * capacity, model_width), jnp.bfloat16)
        .at[slots]
        .set(normed[sources])
    )
    arrived = lax.all_to_all(
        outgoing.reshape(sp_count, local_experts, capacity, model_width),
        "sp",
        split_axis=0,
        concat_axis=0,
        tiled=True,
    )
    piece_rows = lax.all_gather(arrived[None], "tp", axis=0, tiled=True)
    gate_part = jnp.einsum(
        "tsecd,edf->tsecf", piece_rows, gate_weight, preferred_element_type=jnp.float32
    )
    up_part = jnp.einsum(
        "tsecd,edf->tsecf", piece_rows, up_weight, preferred_element_type=jnp.float32
    )
    inner_rows = (jax.nn.silu(gate_part) * up_part).astype(jnp.bfloat16)
    partial_value = jnp.einsum(
        "tsecf,efd->tsecd", inner_rows, down_weight, preferred_element_type=jnp.float32
    )
    reduced = lax.psum_scatter(
        partial_value.astype(jnp.bfloat16), "tp", scatter_dimension=0, tiled=True
    )
    returned = lax.all_to_all(reduced[0], "sp", split_axis=0, concat_axis=0, tiled=True)
    picked = (
        returned.reshape(expert_count * capacity, model_width)[slots]
        .astype(jnp.float32)
        .reshape(rows_here, route_count, model_width)
    )
    moe_sum = jnp.sum(picked * route_weights[:, :, None], axis=1)
    return (updated.astype(jnp.float32) + moe_sum).astype(jnp.bfloat16)


def summed_rows(*terms):
    return sum(term.astype(jnp.float32) for term in terms).astype(jnp.bfloat16)


def near_first(layers):
    return sorted(range(1, layers), key=lambda k: (min(k, layers - k), k))


def fits_balanced(queries, residual, expert_ids, gate_weight, sp_count, tp_count):
    tokens, heads, width = queries.shape
    rows = residual.shape[0]
    held = gate_weight.shape[0]
    if sp_count != 4 or tp_count % 2 or tp_count < 6 or sp_count % heads or width != LANES:
        return False
    sub = rows // (sp_count // heads)
    capacity = row_capacity(rows, expert_ids.shape[1], held * sp_count)
    return (
        sub % 16 == 0
        and tokens % KEY_TILE == 0
        and tokens == rows * tp_count
        and capacity % 16 == 0
        and 3 * held * sp_count <= LANES
    )


def layer(*args):
    queries, residual, expert_ids, gate_weight = args[0], args[6], args[8], args[10]
    chosen = fits_balanced(
        queries, residual, expert_ids, gate_weight, lax.axis_size("sp"), lax.axis_size("tp")
    )
    return (balanced if chosen else shards)(*args)


def solution(mesh):
    placed = (
        P("sp", "tp", None),
        P("sp", "tp", None),
        P("sp", "tp", None),
        P("tp"),
        P(),
        P(),
        P(("sp", "tp"), None),
        P(),
        P(("sp", "tp"), None),
        P(("sp", "tp"), None),
        P("sp", None, "tp"),
        P("sp", None, "tp"),
        P("sp", "tp", None),
    )
    return jax.shard_map(
        layer, mesh=mesh, in_specs=placed, out_specs=P(("sp", "tp"), None), check_vma=False
    )
```
